512 devices in a mesh: fs: 64 (over z, y), tp: 8 (over x, core).
Axes of the slice: x: 4, y: 4, z: 16, core: 2. Of those that a mesh axis runs over, the one named last changes fastest.
Arguments:
- tokens: bfloat16 [16384, 2048], P('fs'), may hold values from -6 to 6
- recurrent_input_gain: bfloat16 [2048], replicated, may hold values from 0.099609375 to 1.8984375
- recurrent_branch_weight: bfloat16 [2048, 1024], P('fs', 'tp'), may hold values from -0.125 to 0.125
- output_gate_weight: bfloat16 [2048, 1024], P('fs', 'tp'), may hold values from -0.125 to 0.125
- filter_taps: bfloat16 [4, 1024], P(None, 'tp'), may hold values from -3 to 3
- retention_gate_blocks: bfloat16 [2, 8, 128, 128], P(None, 'tp'), may hold values from -0.5 to 0.5
- input_gate_blocks: bfloat16 [2, 8, 128, 128], P(None, 'tp'), may hold values from -0.5 to 0.5
- channel_decay_rate: float32 [2, 1024], P(None, 'tp'), may hold values from 0 to 0.008, as said below
- position_log_decay: float32 [2, 16384, 1024], P(None, 'fs', 'tp'), may hold values from -0.7 to 0, as said below
- recurrent_output_weight: bfloat16 [1024, 2048], P('tp', 'fs'), may hold values from -0.1875 to 0.1875
- recurrent_output_gain: bfloat16 [2048], replicated, may hold values from 0.099609375 to 1.8984375
- feedforward_norm_gain: bfloat16 [2048], replicated, may hold values from 0.099609375 to 1.8984375
- feedforward_up_weight: bfloat16 [2048, 8192], P('fs', 'tp'), may hold values from -0.125 to 0.125
- feedforward_down_weight: bfloat16 [8192, 2048], P('tp', 'fs'), may hold values from -0.0625 to 0.0625
- feedforward_output_gain: bfloat16 [2048], replicated, may hold values from 0.099609375 to 1.8984375
Outputs:
- layer_out: bfloat16 [16384, 2048], P('fs')
The draws below stay inside these ranges and needn't reach their ends.
Inputs may be any that keep to these rules, and one draw needn't show every extreme that they name: `channel_decay_rate`: positive rates, one for each channel and direction. `position_log_decay`: zero except at a few positions of each sequence and channel.
All inputs are finite; a program needn't handle non-finite values.
Results may differ from the reference program's by a relative error of at most 0.02.
Values may be sent and summed in bfloat16 or wider, within the bound.
No kernel may reach another device: no remote copies, remote signals or barrier semaphores. Data moves between devices by JAX's collectives and lax.ppermute only.
A program may use at most 128 MiB of HBM per device.

```python
import math
import jax
import jax.numpy as jnp
from jax import lax

D = 2048
RECURRENT_WIDTH = 1024
BLOCK_W = 128
FF = 8192
CONV_W = 4
SEQUENCE_TOKENS = 256
BLOCKS = 8
TOKENS = 16384
N_FS = 64


def draw_channel_decay_rate(key, part):
    keys = jax.random.split(jax.random.fold_in(key, 11), 3)
    slow = jnp.exp(jax.random.uniform(keys[0], (2, RECURRENT_WIDTH), jnp.float32, math.log(0.05), math.log(0.4))) / SEQUENCE_TOKENS
    fast = jnp.exp(jax.random.uniform(keys[1], (2, RECURRENT_WIDTH), jnp.float32, math.log(0.0025), math.log(0.008)))
    share = 0.5
    picked = jax.random.uniform(keys[2], (2, RECURRENT_WIDTH), jnp.float32) < share
    return jnp.where(picked, fast, slow).astype(jnp.float32)


def draw_position_log_decay(key, part):
    keys = jax.random.split(jax.random.fold_in(key, 23), 2)
    chance = jnp.minimum(3.0 / SEQUENCE_TOKENS, 0.5)
    placed = jax.random.uniform(keys[0], (2, TOKENS, RECURRENT_WIDTH), jnp.float32) < chance
    depth = jax.random.uniform(keys[1], (2, TOKENS, RECURRENT_WIDTH), jnp.float32, math.log(0.5), math.log(0.8))
    return jnp.where(placed, depth, 0.0).astype(jnp.float32)


def level_of(own_key, shape, pieces, smallest, largest):
    level, own = 1.0, jax.random.fold_in(own_key, 6)
    for axis_at, blocks in pieces:
        heights = jnp.exp(jax.random.uniform(jax.random.fold_in(own, axis_at), (blocks,), jnp.float32, smallest / len(pieces), largest / len(pieces)))
        level = level * jnp.repeat(heights, shape[axis_at] // blocks).reshape([-1 if axis == axis_at else 1 for axis in range(len(shape))])
    return level


def centred(rng, extent, width, limit, cuts=(), held_as=jnp.bfloat16):
    entries = jax.random.normal(rng, extent, jnp.float32) * width
    if len(cuts) > 0:
        entries = level_of(rng, extent, cuts, -0.22, 0.18) * entries
    return jnp.clip(entries, min=-limit, max=limit).astype(held_as)


def setup_inputs(seed: int = 0) -> dict:
    streams_of = jax.random.split(jax.random.key(seed), 16)
    tokens = centred(streams_of[0], (TOKENS, D), 1.0, 6.0, ((0, 64),))
    recurrent_input_gain = jnp.clip(1.0 + 0.18 * jax.random.normal(streams_of[1], (D,), jnp.float32), 0.099609375, 1.8984375).astype(jnp.bfloat16)
    recurrent_branch_weight = centred(streams_of[2], (D, RECURRENT_WIDTH), D ** -0.5, 0.125, ((0, 64), (1, 8)))
    output_gate_weight = centred(streams_of[3], (D, RECURRENT_WIDTH), D ** -0.5, 0.125, ((0, 64), (1, 8)))
    filter_taps = centred(streams_of[4], (CONV_W, RECURRENT_WIDTH), CONV_W ** -0.5, 3.0, ((1, 8),))
    retention_gate_blocks = centred(streams_of[5], (2, BLOCKS, BLOCK_W, BLOCK_W), BLOCK_W ** -0.5, 0.5, ((1, 8),))
    input_gate_blocks = centred(streams_of[6], (2, BLOCKS, BLOCK_W, BLOCK_W), BLOCK_W ** -0.5, 0.5, ((1, 8),))
    channel_decay_rate = draw_channel_decay_rate(jax.random.fold_in(streams_of[15], 71), 0)
    position_log_decay = draw_position_log_decay(jax.random.fold_in(streams_of[15], 71), 0)
    recurrent_output_weight = centred(streams_of[9], (RECURRENT_WIDTH, D), RECURRENT_WIDTH ** -0.5, 0.1875, ((0, 8), (1, 64)))
    recurrent_output_gain = jnp.clip(1.0 + 0.18 * jax.random.normal(streams_of[10], (D,), jnp.float32), 0.099609375, 1.8984375).astype(jnp.bfloat16)
    feedforward_norm_gain = jnp.clip(1.0 + 0.18 * jax.random.normal(streams_of[11], (D,), jnp.float32), 0.099609375, 1.8984375).astype(jnp.bfloat16)
    feedforward_up_weight = centred(streams_of[12], (D, FF), D ** -0.5, 0.125, ((0, 64), (1, 8)))
    feedforward_down_weight = centred(streams_of[13], (FF, D), FF ** -0.5, 0.0625, ((0, 8), (1, 64)))
    feedforward_output_gain = jnp.clip(1.0 + 0.18 * jax.random.normal(streams_of[14], (D,), jnp.float32), 0.099609375, 1.8984375).astype(jnp.bfloat16)
    return dict(tokens=tokens, recurrent_input_gain=recurrent_input_gain, recurrent_branch_weight=recurrent_branch_weight, output_gate_weight=output_gate_weight, filter_taps=filter_taps, retention_gate_blocks=retention_gate_blocks, input_gate_blocks=input_gate_blocks, channel_decay_rate=channel_decay_rate, position_log_decay=position_log_decay, recurrent_output_weight=recurrent_output_weight, recurrent_output_gain=recurrent_output_gain, feedforward_norm_gain=feedforward_norm_gain, feedforward_up_weight=feedforward_up_weight, feedforward_down_weight=feedforward_down_weight, feedforward_output_gain=feedforward_output_gain)


EPS = 1e-06
GATE_STEEPNESS = 8.0

def root_norm(values, gain):
    return values * lax.rsqrt(lax.optimization_barrier(jnp.mean(values * values, axis=-1, keepdims=True)) + EPS) * gain.astype(jnp.float32)

def combine(earlier, later):
    return (earlier[0] * later[0], later[0] * earlier[1] + later[1])

def centred_conv(signal, taps):
    length = signal.shape[0]
    width_taps = taps.shape[0]
    left_pad = width_taps // 2
    padded = jnp.pad(signal.astype(jnp.float32), ((left_pad, width_taps - 1 - left_pad), (0, 0)))
    total = jnp.zeros(signal.shape, jnp.float32)
    for offset in range(width_taps):
        total = total + padded[offset:offset + length] * taps[offset].astype(jnp.float32)
    return total.astype(jnp.bfloat16)

def block_map(signal, matrices):
    block_width = matrices.shape[-1]
    shaped = signal.astype(jnp.float32).reshape(signal.shape[0], matrices.shape[0], block_width)
    mapped = jnp.einsum('tnc,ncd->tnd', shaped, matrices.astype(jnp.float32))
    return mapped.reshape(signal.shape)

def linear_recurrence(convolved_output, retention_matrices, input_gate_matrices, decay_rate_row, decay_extra_block, reversed_scan):
    retention_gate = jax.nn.sigmoid(block_map(convolved_output, retention_matrices))
    admit = jax.nn.sigmoid(block_map(convolved_output, input_gate_matrices))
    logarithm_decay = -GATE_STEEPNESS * retention_gate * decay_rate_row[None, :] + decay_extra_block
    decay = jnp.exp(logarithm_decay)
    drive = jnp.sqrt(-jnp.expm1(2.0 * logarithm_decay)) * (admit * convolved_output.astype(jnp.float32))
    _, state = lax.associative_scan(combine, (decay, drive), reverse=reversed_scan, axis=0)
    return state

def reference(tokens, recurrent_input_gain, recurrent_branch_weight, output_gate_weight, filter_taps, retention_gate_blocks, input_gate_blocks, channel_decay_rate, position_log_decay, recurrent_output_weight, recurrent_output_gain, feedforward_norm_gain, feedforward_up_weight, feedforward_down_weight, feedforward_output_gain):

    def single_sequence(scan_operands):
        token_row_block, decay_extra_rows = scan_operands
        normed = root_norm(token_row_block.astype(jnp.float32), recurrent_input_gain).astype(jnp.bfloat16)
        recur_in = jnp.dot(normed, recurrent_branch_weight, preferred_element_type=jnp.float32).astype(jnp.bfloat16)
        gate_in = lax.optimization_barrier(jnp.dot(normed, output_gate_weight, preferred_element_type=jnp.float32).astype(jnp.bfloat16))
        convolved_output = lax.optimization_barrier(centred_conv(recur_in, filter_taps))
        forward_sweep = linear_recurrence(convolved_output, retention_gate_blocks[0], input_gate_blocks[0], channel_decay_rate[0], decay_extra_rows[0], False)
        backward_sweep = linear_recurrence(convolved_output, retention_gate_blocks[1], input_gate_blocks[1], channel_decay_rate[1], decay_extra_rows[1], True)
        hidden = ((forward_sweep + backward_sweep) * jax.nn.gelu(gate_in.astype(jnp.float32))).astype(jnp.bfloat16)
        mixed = jnp.dot(hidden, recurrent_output_weight, preferred_element_type=jnp.float32)
        stream = lax.optimization_barrier((token_row_block.astype(jnp.float32) + root_norm(mixed, recurrent_output_gain)).astype(jnp.bfloat16))
        normed_ff = root_norm(stream.astype(jnp.float32), feedforward_norm_gain).astype(jnp.bfloat16)
        lifted = jnp.square(jax.nn.relu(jnp.dot(normed_ff, feedforward_up_weight, preferred_element_type=jnp.float32))).astype(jnp.bfloat16)
        lowered = jnp.dot(lifted, feedforward_down_weight, preferred_element_type=jnp.float32)
        return (stream.astype(jnp.float32) + root_norm(lowered, feedforward_output_gain)).astype(jnp.bfloat16)
    stacked_directions = tokens.reshape(N_FS, SEQUENCE_TOKENS, D)
    decay_extras = position_log_decay.reshape(2, N_FS, SEQUENCE_TOKENS, RECURRENT_WIDTH).transpose(1, 0, 2, 3)
    final_result = lax.map(single_sequence, (stacked_directions, decay_extras))
    return final_result.reshape(TOKENS, D)
```

```python
import jax
import jax.numpy as jnp
from jax import lax
from jax.sharding import Mesh
from jax.sharding import PartitionSpec as P

FS = ("zh", "zl", "y")
Z = ("zh", "zl")
TP = ("x", "c")


EPS = 1e-06
GATE_STEEPNESS = 8.0


def spread(array, axis):
    copies = jnp.broadcast_to(array, (lax.axis_size(axis), *array.shape))
    return lax.all_to_all(copies, axis, split_axis=0, concat_axis=0, tiled=True)


def mixer_weights(array):
    width = array.shape[-1]
    pieces = spread(spread(spread(array, "zh"), "zl"), "y")
    return jnp.transpose(pieces, (2, 1, 0, 3, 4)).reshape(-1, width)


def feedforward_weights(array):
    near = spread(array, "y").reshape(-1, array.shape[-1])
    return lax.all_gather(near, Z, axis=0, tiled=True)


def summed_rows(partial):
    cores, wide = lax.axis_size("c"), lax.axis_size("x")
    rows, width = partial.shape
    halves = partial.astype(jnp.bfloat16).reshape(cores, rows // cores, width)
    pair = lax.all_to_all(halves, "c", split_axis=0, concat_axis=0, tiled=True)
    half = jnp.sum(pair.astype(jnp.float32), axis=0).astype(jnp.bfloat16)
    quarters = half.reshape(wide, rows // (cores * wide), width)
    several = lax.all_to_all(quarters, "x", split_axis=0, concat_axis=0, tiled=True)
    return jnp.sum(several.astype(jnp.float32), axis=0)


def all_rows(part):
    return spread(spread(part, "x"), "c").reshape(-1, part.shape[-1])


def root_norm(values, gain):
    return (
        values
        * lax.rsqrt(jnp.mean(values * values, axis=-1, keepdims=True) + EPS)
        * gain.astype(jnp.float32)
    )


def combine(earlier, later):
    return (earlier[0] * later[0], later[0] * earlier[1] + later[1])


def centred_conv(signal, taps):
    length = signal.shape[0]
    width_taps = taps.shape[0]
    left_pad = width_taps // 2
    padded = jnp.pad(signal.astype(jnp.float32), ((left_pad, width_taps - 1 - left_pad), (0, 0)))
    total = jnp.zeros(signal.shape, jnp.float32)
    for offset in range(width_taps):
        total = total + padded[offset : offset + length] * taps[offset].astype(jnp.float32)
    return total.astype(jnp.bfloat16)


def block_map(signal, matrices):
    block_width = matrices.shape[-1]
    shaped = signal.reshape(signal.shape[0], matrices.shape[0], block_width)
    mapped = jnp.einsum("tnc,ncd->tnd", shaped, matrices, preferred_element_type=jnp.float32)
    return mapped.reshape(signal.shape)


def linear_recurrence(
    convolved_output,
    retention_matrices,
    input_gate_matrices,
    decay_rate_row,
    decay_extra_block,
    reversed_scan,
):
    retention_gate = jax.nn.sigmoid(block_map(convolved_output, retention_matrices))
    admit = jax.nn.sigmoid(block_map(convolved_output, input_gate_matrices))
    logarithm_decay = -GATE_STEEPNESS * retention_gate * decay_rate_row[None, :] + decay_extra_block
    decay = jnp.exp(logarithm_decay)
    drive = jnp.sqrt(-jnp.expm1(2.0 * logarithm_decay)) * (
        admit * convolved_output.astype(jnp.float32)
    )
    _, state = lax.associative_scan(combine, (decay, drive), reverse=reversed_scan, axis=0)
    return state


def per_device(
    tokens,
    recurrent_input_gain,
    recurrent_branch_weight,
    output_gate_weight,
    filter_taps,
    retention_gate_blocks,
    input_gate_blocks,
    channel_decay_rate,
    position_log_decay,
    recurrent_output_weight,
    recurrent_output_gain,
    feedforward_norm_gain,
    feedforward_up_weight,
    feedforward_down_weight,
    feedforward_output_gain,
):
    mixer = mixer_weights(
        jnp.concatenate(
            (recurrent_branch_weight, output_gate_weight, recurrent_output_weight.T), axis=1
        )
    )
    forward = feedforward_weights(
        jnp.concatenate((feedforward_up_weight, feedforward_down_weight.T), axis=1)
    )
    channels = recurrent_branch_weight.shape[1]
    hidden_units = feedforward_up_weight.shape[1]
    normed = root_norm(tokens.astype(jnp.float32), recurrent_input_gain).astype(jnp.bfloat16)
    recur_sum = jnp.dot(normed, mixer[:, :channels], preferred_element_type=jnp.float32)
    gate_sum = jnp.dot(
        normed, mixer[:, channels : 2 * channels], preferred_element_type=jnp.float32
    )
    recur_in = recur_sum.astype(jnp.bfloat16)
    gate_in = lax.optimization_barrier(gate_sum.astype(jnp.bfloat16))
    convolved_output = lax.optimization_barrier(centred_conv(recur_in, filter_taps))
    forward_sweep = linear_recurrence(
        convolved_output,
        retention_gate_blocks[0],
        input_gate_blocks[0],
        channel_decay_rate[0],
        position_log_decay[0],
        False,
    )
    backward_sweep = linear_recurrence(
        convolved_output,
        retention_gate_blocks[1],
        input_gate_blocks[1],
        channel_decay_rate[1],
        position_log_decay[1],
        True,
    )
    hidden = ((forward_sweep + backward_sweep) * jax.nn.gelu(gate_in.astype(jnp.float32))).astype(
        jnp.bfloat16
    )
    across = (((1,), (1,)), ((), ()))
    partial_value = lax.dot_general(
        hidden, mixer[:, 2 * channels :], across, preferred_element_type=jnp.float32
    )
    mixed = summed_rows(partial_value)
    share = mixed.shape[0]
    place = lax.axis_index("c") * lax.axis_size("x") + lax.axis_index("x")
    own = lax.dynamic_slice_in_dim(tokens, place * share, share, axis=0)
    stream = lax.optimization_barrier(
        (own.astype(jnp.float32) + root_norm(mixed, recurrent_output_gain)).astype(jnp.bfloat16)
    )
    normed_ff = all_rows(
        root_norm(stream.astype(jnp.float32), feedforward_norm_gain).astype(jnp.bfloat16)
    )
    lifted_sum = jnp.dot(normed_ff, forward[:, :hidden_units], preferred_element_type=jnp.float32)
    lifted = jnp.square(jax.nn.relu(lifted_sum)).astype(jnp.bfloat16)
    lowered_part = lax.dot_general(
        lifted, forward[:, hidden_units:], across, preferred_element_type=jnp.float32
    )
    lowered = summed_rows(lowered_part)
    return all_rows(
        (stream.astype(jnp.float32) + root_norm(lowered, feedforward_output_gain)).astype(
            jnp.bfloat16
        )
    )


def solution(mesh):
    split = Mesh(mesh.devices.reshape(4, 4, 4, 4, 2), ("zh", "zl", "y", "x", "c"))
    placed = (
        P(FS, None),
        P(),
        P(FS, TP),
        P(FS, TP),
        P(None, TP),
        P(None, TP, None, None),
        P(None, TP, None, None),
        P(None, TP),
        P(None, FS, TP),
        P(TP, FS),
        P(),
        P(),
        P(FS, TP),
        P(TP, FS),
        P(),
    )
    return jax.shard_map(
        per_device, mesh=split, in_specs=placed, out_specs=P(FS, None), check_vma=False
    )
```

```python
import jax
import jax.numpy as jnp
from jax import lax
from jax.sharding import Mesh
from jax.sharding import PartitionSpec as P

FS = ("zh", "zl", "y")
Z = ("zh", "zl")
TP = ("x", "c")


EPS = 1e-06
GATE_STEEPNESS = 8.0


def spread(array, axis):
    copies = jnp.broadcast_to(array, (lax.axis_size(axis), *array.shape))
    return lax.all_to_all(copies, axis, split_axis=0, concat_axis=0, tiled=True)


def in_order(pieces):
    along, deep = pieces.shape[0], lax.axis_size(Z)
    width = pieces.shape[-1]
    return jnp.transpose(pieces.reshape(along, deep, -1, width), (1, 0, 2, 3)).reshape(-1, width)


def from_others(array, axis):
    size = lax.axis_size(axis)
    here = lax.axis_index(axis)
    out = jnp.zeros((size, *array.shape), array.dtype)
    for step in range(size):
        ring = [(i, (i + step) % size) for i in range(size)]
        piece = lax.ppermute(array, axis, ring) if step else array
        out = lax.dynamic_update_index_in_dim(out, piece, (here - step) % size, 0)
    return out


def summed_rows(partial):
    cores, wide = lax.axis_size("c"), lax.axis_size("x")
    rows, width = partial.shape
    halves = partial.astype(jnp.bfloat16).reshape(cores, rows // cores, width)
    pair = lax.all_to_all(halves, "c", split_axis=0, concat_axis=0, tiled=True)
    half = jnp.sum(pair.astype(jnp.float32), axis=0).astype(jnp.bfloat16)
    quarters = half.reshape(wide, rows // (cores * wide), width)
    several = lax.all_to_all(quarters, "x", split_axis=0, concat_axis=0, tiled=True)
    return jnp.sum(several.astype(jnp.float32), axis=0)


def all_rows(part):
    return spread(spread(part, "x"), "c").reshape(-1, part.shape[-1])


def root_norm(values, gain):
    return (
        values
        * lax.rsqrt(jnp.mean(values * values, axis=-1, keepdims=True) + EPS)
        * gain.astype(jnp.float32)
    )


def combine(earlier, later):
    return (earlier[0] * later[0], later[0] * earlier[1] + later[1])


def centred_conv(signal, taps):
    length = signal.shape[0]
    width_taps = taps.shape[0]
    left_pad = width_taps // 2
    padded = jnp.pad(signal.astype(jnp.float32), ((left_pad, width_taps - 1 - left_pad), (0, 0)))
    total = jnp.zeros(signal.shape, jnp.float32)
    for offset in range(width_taps):
        total = total + padded[offset : offset + length] * taps[offset].astype(jnp.float32)
    return total.astype(jnp.bfloat16)


def block_map(signal, matrices):
    block_width = matrices.shape[-1]
    shaped = signal.reshape(signal.shape[0], matrices.shape[0], block_width)
    mapped = jnp.einsum("tnc,ncd->tnd", shaped, matrices, preferred_element_type=jnp.float32)
    return mapped.reshape(signal.shape)


def linear_recurrence(
    convolved_output,
    retention_matrices,
    input_gate_matrices,
    decay_rate_row,
    decay_extra_block,
    reversed_scan,
):
    retention_gate = jax.nn.sigmoid(block_map(convolved_output, retention_matrices))
    admit = jax.nn.sigmoid(block_map(convolved_output, input_gate_matrices))
    logarithm_decay = -GATE_STEEPNESS * retention_gate * decay_rate_row[None, :] + decay_extra_block
    decay = jnp.exp(logarithm_decay)
    drive = jnp.sqrt(-jnp.expm1(2.0 * logarithm_decay)) * (
        admit * convolved_output.astype(jnp.float32)
    )
    _, state = lax.associative_scan(combine, (decay, drive), reverse=reversed_scan, axis=0)
    return state


def per_device(
    tokens,
    recurrent_input_gain,
    recurrent_branch_weight,
    output_gate_weight,
    filter_taps,
    retention_gate_blocks,
    input_gate_blocks,
    channel_decay_rate,
    position_log_decay,
    recurrent_output_weight,
    recurrent_output_gain,
    feedforward_norm_gain,
    feedforward_up_weight,
    feedforward_down_weight,
    feedforward_output_gain,
):
    channels = recurrent_branch_weight.shape[1]
    hidden_units = feedforward_up_weight.shape[1]
    early = hidden_units // 2
    down_rows = feedforward_down_weight.T
    near = spread(jnp.concatenate((feedforward_up_weight, down_rows[:, :early]), axis=1), "y")
    forward = lax.all_gather(near.reshape(-1, near.shape[-1]), Z, axis=0, tiled=True)
    own_rows = jnp.concatenate(
        (
            recurrent_branch_weight,
            output_gate_weight,
            recurrent_output_weight.T,
            down_rows[:, early:],
        ),
        axis=1,
    )
    own_rows, _ = lax.optimization_barrier((own_rows, near))
    column = lax.all_gather(own_rows, Z, axis=0, tiled=True)
    mixer = spread(column[:, : 3 * channels], "y")
    late_rows, mixer = lax.optimization_barrier((column[:, 3 * channels :], mixer))
    late = from_others(late_rows, "y")
    mixer = in_order(mixer)
    normed = root_norm(tokens.astype(jnp.float32), recurrent_input_gain).astype(jnp.bfloat16)
    recur_sum = jnp.dot(normed, mixer[:, :channels], preferred_element_type=jnp.float32)
    gate_sum = jnp.dot(
        normed, mixer[:, channels : 2 * channels], preferred_element_type=jnp.float32
    )
    recur_in = recur_sum.astype(jnp.bfloat16)
    gate_in = lax.optimization_barrier(gate_sum.astype(jnp.bfloat16))
    convolved_output = lax.optimization_barrier(centred_conv(recur_in, filter_taps))
    forward_sweep = linear_recurrence(
        convolved_output,
        retention_gate_blocks[0],
        input_gate_blocks[0],
        channel_decay_rate[0],
        position_log_decay[0],
        False,
    )
    backward_sweep = linear_recurrence(
        convolved_output,
        retention_gate_blocks[1],
        input_gate_blocks[1],
        channel_decay_rate[1],
        position_log_decay[1],
        True,
    )
    hidden = ((forward_sweep + backward_sweep) * jax.nn.gelu(gate_in.astype(jnp.float32))).astype(
        jnp.bfloat16
    )
    across = (((1,), (1,)), ((), ()))
    partial_value = lax.dot_general(
        hidden, mixer[:, 2 * channels :], across, preferred_element_type=jnp.float32
    )
    share = tokens.shape[0] // lax.axis_size(TP)
    place = lax.axis_index("c") * lax.axis_size("x") + lax.axis_index("x")
    own = lax.dynamic_slice_in_dim(tokens, place * share, share, axis=0)
    own, partial_value = lax.optimization_barrier((own, partial_value.astype(jnp.bfloat16)))
    mixed = summed_rows(partial_value)
    stream = lax.optimization_barrier(
        (own.astype(jnp.float32) + root_norm(mixed, recurrent_output_gain)).astype(jnp.bfloat16)
    )
    normed_ff = all_rows(
        root_norm(stream.astype(jnp.float32), feedforward_norm_gain).astype(jnp.bfloat16)
    )
    lifted_sum = jnp.dot(normed_ff, forward[:, :hidden_units], preferred_element_type=jnp.float32)
    lifted = jnp.square(jax.nn.relu(lifted_sum)).astype(jnp.bfloat16)
    lowered_part = lax.dot_general(
        lifted[:, :early], forward[:, hidden_units:], across, preferred_element_type=jnp.float32
    ) + lax.dot_general(
        lifted[:, early:], in_order(late), across, preferred_element_type=jnp.float32
    )
    lowered = summed_rows(lowered_part)
    return all_rows(
        (stream.astype(jnp.float32) + root_norm(lowered, feedforward_output_gain)).astype(
            jnp.bfloat16
        )
    )


def solution(mesh):
    split = Mesh(mesh.devices.reshape(4, 4, 4, 4, 2), ("zh", "zl", "y", "x", "c"))
    placed = (
        P(FS, None),
        P(),
        P(FS, TP),
        P(FS, TP),
        P(None, TP),
        P(None, TP, None, None),
        P(None, TP, None, None),
        P(None, TP),
        P(None, FS, TP),
        P(TP, FS),
        P(),
        P(),
        P(FS, TP),
        P(TP, FS),
        P(),
    )
    return jax.shard_map(
        per_device, mesh=split, in_specs=placed, out_specs=P(FS, None), check_vma=False
    )
```

```python
import jax
import jax.numpy as jnp
from jax import lax
from jax.sharding import Mesh
from jax.sharding import PartitionSpec as P

FS = ("zh", "zl", "y")
Z = ("zh", "zl")
TP = ("x", "c")


EPS = 1e-06
GATE_STEEPNESS = 8.0


def spread(array, axis):
    copies = jnp.broadcast_to(array, (lax.axis_size(axis), *array.shape))
    return lax.all_to_all(copies, axis, split_axis=0, concat_axis=0, tiled=True)


def mixer_weights(array):
    width = array.shape[-1]
    pieces = spread(spread(spread(array, "zh"), "zl"), "y")
    return jnp.transpose(pieces, (2, 1, 0, 3, 4)).reshape(-1, width)


def feedforward_weights(array):
    near = spread(array, "y").reshape(-1, array.shape[-1])
    return lax.all_gather(near, Z, axis=0, tiled=True)


def summed_rows(partial):
    cores, wide = lax.axis_size("c"), lax.axis_size("x")
    rows, width = partial.shape
    halves = partial.astype(jnp.bfloat16).reshape(cores, rows // cores, width)
    pair = lax.all_to_all(halves, "c", split_axis=0, concat_axis=0, tiled=True)
    half = jnp.sum(pair.astype(jnp.float32), axis=0).astype(jnp.bfloat16)
    quarters = half.reshape(wide, rows // (cores * wide), width)
    several = lax.all_to_all(quarters, "x", split_axis=0, concat_axis=0, tiled=True)
    return jnp.sum(several.astype(jnp.float32), axis=0)


def all_rows(part):
    return spread(spread(part, "x"), "c").reshape(-1, part.shape[-1])


def root_norm(values, gain):
    return (
        values
        * lax.rsqrt(jnp.mean(values * values, axis=-1, keepdims=True) + EPS)
        * gain.astype(jnp.float32)
    )


def combine(earlier, later):
    return (earlier[0] * later[0], later[0] * earlier[1] + later[1])


def centred_conv(signal, taps):
    length = signal.shape[0]
    width_taps = taps.shape[0]
    left_pad = width_taps // 2
    padded = jnp.pad(signal.astype(jnp.float32), ((left_pad, width_taps - 1 - left_pad), (0, 0)))
    total = jnp.zeros(signal.shape, jnp.float32)
    for offset in range(width_taps):
        total = total + padded[offset : offset + length] * taps[offset].astype(jnp.float32)
    return total.astype(jnp.bfloat16)


def block_map(signal, matrices):
    block_width = matrices.shape[-1]
    shaped = signal.reshape(signal.shape[0], matrices.shape[0], block_width)
    mapped = jnp.einsum("tnc,ncd->tnd", shaped, matrices, preferred_element_type=jnp.float32)
    return mapped.reshape(signal.shape)


def linear_recurrence(
    convolved_output,
    retention_matrices,
    input_gate_matrices,
    decay_rate_row,
    decay_extra_block,
    reversed_scan,
):
    retention_gate = jax.nn.sigmoid(block_map(convolved_output, retention_matrices))
    admit = jax.nn.sigmoid(block_map(convolved_output, input_gate_matrices))
    logarithm_decay = -GATE_STEEPNESS * retention_gate * decay_rate_row[None, :] + decay_extra_block
    decay = jnp.exp(logarithm_decay)
    drive = jnp.sqrt(-jnp.expm1(2.0 * logarithm_decay)) * (
        admit * convolved_output.astype(jnp.float32)
    )
    _, state = lax.associative_scan(combine, (decay, drive), reverse=reversed_scan, axis=0)
    return state


def per_device(
    tokens,
    recurrent_input_gain,
    recurrent_branch_weight,
    output_gate_weight,
    filter_taps,
    retention_gate_blocks,
    input_gate_blocks,
    channel_decay_rate,
    position_log_decay,
    recurrent_output_weight,
    recurrent_output_gain,
    feedforward_norm_gain,
    feedforward_up_weight,
    feedforward_down_weight,
    feedforward_output_gain,
):
    mixer = mixer_weights(
        jnp.concatenate(
            (recurrent_branch_weight, output_gate_weight, recurrent_output_weight.T), axis=1
        )
    )
    forward = feedforward_weights(
        jnp.concatenate((feedforward_up_weight, feedforward_down_weight.T), axis=1)
    )
    channels = recurrent_branch_weight.shape[1]
    hidden_units = feedforward_up_weight.shape[1]
    normed = root_norm(tokens.astype(jnp.float32), recurrent_input_gain).astype(jnp.bfloat16)
    recur_sum = jnp.dot(normed, mixer[:, :channels], preferred_element_type=jnp.float32)
    gate_sum = jnp.dot(
        normed, mixer[:, channels : 2 * channels], preferred_element_type=jnp.float32
    )
    recur_in = recur_sum.astype(jnp.bfloat16)
    gate_in = lax.optimization_barrier(gate_sum.astype(jnp.bfloat16))
    convolved_output = lax.optimization_barrier(centred_conv(recur_in, filter_taps))
    forward_sweep = linear_recurrence(
        convolved_output,
        retention_gate_blocks[0],
        input_gate_blocks[0],
        channel_decay_rate[0],
        position_log_decay[0],
        False,
    )
    backward_sweep = linear_recurrence(
        convolved_output,
        retention_gate_blocks[1],
        input_gate_blocks[1],
        channel_decay_rate[1],
        position_log_decay[1],
        True,
    )
    hidden = ((forward_sweep + backward_sweep) * jax.nn.gelu(gate_in.astype(jnp.float32))).astype(
        jnp.bfloat16
    )
    across = (((1,), (1,)), ((), ()))
    partial_value = lax.dot_general(
        hidden, mixer[:, 2 * channels :], across, preferred_element_type=jnp.float32
    )
    share = tokens.shape[0] // lax.axis_size(TP)
    place = lax.axis_index("c") * lax.axis_size("x") + lax.axis_index("x")
    own = lax.dynamic_slice_in_dim(tokens, place * share, share, axis=0)
    own, partial_value, mixer_gain, norm_gain, out_gain = lax.optimization_barrier(
        (
            own,
            partial_value.astype(jnp.bfloat16),
            recurrent_output_gain.astype(jnp.float32),
            feedforward_norm_gain.astype(jnp.float32),
            feedforward_output_gain.astype(jnp.float32),
        )
    )
    mixed = summed_rows(partial_value)
    stream = lax.optimization_barrier(
        (own.astype(jnp.float32) + root_norm(mixed, mixer_gain)).astype(jnp.bfloat16)
    )
    normed_ff = all_rows(
        root_norm(stream.astype(jnp.float32), norm_gain).astype(jnp.bfloat16)
    )
    lifted_sum = jnp.dot(normed_ff, forward[:, :hidden_units], preferred_element_type=jnp.float32)
    lifted = jnp.square(jax.nn.relu(lifted_sum)).astype(jnp.bfloat16)
    lowered_part = lax.dot_general(
        lifted, forward[:, hidden_units:], across, preferred_element_type=jnp.float32
    )
    lowered = summed_rows(lowered_part)
    return all_rows(
        (stream.astype(jnp.float32) + root_norm(lowered, out_gain)).astype(
            jnp.bfloat16
        )
    )


def solution(mesh):
    split = Mesh(mesh.devices.reshape(4, 4, 4, 4, 2), ("zh", "zl", "y", "x", "c"))
    placed = (
        P(FS, None),
        P(),
        P(FS, TP),
        P(FS, TP),
        P(None, TP),
        P(None, TP, None, None),
        P(None, TP, None, None),
        P(None, TP),
        P(None, FS, TP),
        P(TP, FS),
        P(),
        P(),
        P(FS, TP),
        P(TP, FS),
        P(),
    )
    return jax.shard_map(
        per_device, mesh=split, in_specs=placed, out_specs=P(FS, None), check_vma=False
    )
```

```python
import jax
import jax.numpy as jnp
from jax import lax
from jax.experimental import pallas as pl
from jax.experimental.pallas import tpu as pltpu
from jax.sharding import Mesh
from jax.sharding import PartitionSpec as P

FS = ("zh", "zl", "y")
Z = ("zh", "zl")
TP = ("x", "c")


EPS = 1e-06
GATE_STEEPNESS = 8.0


def spread(array, axis):
    copies = jnp.broadcast_to(array, (lax.axis_size(axis), *array.shape))
    return lax.all_to_all(copies, axis, split_axis=0, concat_axis=0, tiled=True)


def mixer_weights(array):
    rows, width = array.shape
    pieces = spread(lax.all_gather(array, Z, axis=0, tiled=True), "y")
    pieces = pieces.reshape(pieces.shape[0], -1, rows, width)
    return jnp.transpose(pieces, (1, 0, 2, 3)).reshape(-1, width)


def feedforward_weights(array):
    near = spread(array, "y").reshape(-1, array.shape[-1])
    return lax.all_gather(near, Z, axis=0, tiled=True)


def summed_rows(partial):
    cores, wide = lax.axis_size("c"), lax.axis_size("x")
    rows, width = partial.shape
    halves = partial.astype(jnp.bfloat16).reshape(cores, rows // cores, width)
    pair = lax.all_to_all(halves, "c", split_axis=0, concat_axis=0, tiled=True)
    half = jnp.sum(pair.astype(jnp.float32), axis=0).astype(jnp.bfloat16)
    quarters = half.reshape(wide, rows // (cores * wide), width)
    several = lax.all_to_all(quarters, "x", split_axis=0, concat_axis=0, tiled=True)
    return jnp.sum(several.astype(jnp.float32), axis=0)


def all_rows(part):
    return spread(spread(part, "x"), "c").reshape(-1, part.shape[-1])


def root_norm(values, gain):
    return (
        values
        * lax.rsqrt(jnp.mean(values * values, axis=-1, keepdims=True) + EPS)
        * gain.astype(jnp.float32)
    )


def swept(decay, drive, backward):
    length = decay.shape[0]
    place = lax.broadcasted_iota(jnp.int32, decay.shape, 0)
    step = 1
    while step < length:
        if step % 8:
            turn = length - step if backward else step
            inside = place < length - step if backward else place >= step
            far_decay = jnp.where(inside, pltpu.roll(decay, turn, 0), 1.0)
            far_drive = jnp.where(inside, pltpu.roll(drive, turn, 0), 0.0)
        else:
            one = jnp.ones((step, decay.shape[1]), jnp.float32)
            if backward:
                far_decay = jnp.concatenate((decay[step:], one), axis=0)
                far_drive = jnp.concatenate((drive[step:], 0.0 * one), axis=0)
            else:
                far_decay = jnp.concatenate((one, decay[:-step]), axis=0)
                far_drive = jnp.concatenate((0.0 * one, drive[:-step]), axis=0)
        drive = drive + decay * far_drive
        decay = decay * far_decay
        step *= 2
    return drive


def hidden_kernel(decay_0, drive_0, decay_1, drive_1, gate, out):
    state = swept(decay_0[...], drive_0[...], False) + swept(decay_1[...], drive_1[...], True)
    out[...] = (state * jax.nn.gelu(gate[...].astype(jnp.float32))).astype(out.dtype)


def centred_conv(signal, taps):
    length = signal.shape[0]
    width_taps = taps.shape[0]
    left_pad = width_taps // 2
    padded = jnp.pad(signal.astype(jnp.float32), ((left_pad, width_taps - 1 - left_pad), (0, 0)))
    total = jnp.zeros(signal.shape, jnp.float32)
    for offset in range(width_taps):
        total = total + padded[offset : offset + length] * taps[offset].astype(jnp.float32)
    return total.astype(jnp.bfloat16)


def block_map(signal, matrices):
    block_width = matrices.shape[-1]
    shaped = signal.reshape(signal.shape[0], matrices.shape[0], block_width)
    mapped = jnp.einsum("tnc,ncd->tnd", shaped, matrices, preferred_element_type=jnp.float32)
    return mapped.reshape(signal.shape)


def decay_and_drive(
    convolved_output, retention_matrices, input_gate_matrices, decay_rate_row, decay_extra_block
):
    retention_gate = jax.nn.sigmoid(block_map(convolved_output, retention_matrices))
    admit = jax.nn.sigmoid(block_map(convolved_output, input_gate_matrices))
    logarithm_decay = -GATE_STEEPNESS * retention_gate * decay_rate_row[None, :] + decay_extra_block
    decay = jnp.exp(logarithm_decay)
    drive = jnp.sqrt(-jnp.expm1(2.0 * logarithm_decay)) * (
        admit * convolved_output.astype(jnp.float32)
    )
    return decay, drive


def per_device(
    tokens,
    recurrent_input_gain,
    recurrent_branch_weight,
    output_gate_weight,
    filter_taps,
    retention_gate_blocks,
    input_gate_blocks,
    channel_decay_rate,
    position_log_decay,
    recurrent_output_weight,
    recurrent_output_gain,
    feedforward_norm_gain,
    feedforward_up_weight,
    feedforward_down_weight,
    feedforward_output_gain,
):
    mixer = mixer_weights(
        jnp.concatenate(
            (recurrent_branch_weight, output_gate_weight, recurrent_output_weight.T), axis=1
        )
    )
    forward = feedforward_weights(
        jnp.concatenate((feedforward_up_weight, feedforward_down_weight.T), axis=1)
    )
    channels = recurrent_branch_weight.shape[1]
    hidden_units = feedforward_up_weight.shape[1]
    normed = root_norm(tokens.astype(jnp.float32), recurrent_input_gain).astype(jnp.bfloat16)
    recur_sum = jnp.dot(normed, mixer[:, :channels], preferred_element_type=jnp.float32)
    gate_sum = jnp.dot(
        normed, mixer[:, channels : 2 * channels], preferred_element_type=jnp.float32
    )
    recur_in = recur_sum.astype(jnp.bfloat16)
    gate_in = lax.optimization_barrier(gate_sum.astype(jnp.bfloat16))
    convolved_output = lax.optimization_barrier(centred_conv(recur_in, filter_taps))
    directions = []
    for way in range(2):
        directions += decay_and_drive(
            convolved_output,
            retention_gate_blocks[way],
            input_gate_blocks[way],
            channel_decay_rate[way],
            position_log_decay[way],
        )
    hidden = pl.pallas_call(
        hidden_kernel, out_shape=jax.ShapeDtypeStruct(gate_in.shape, jnp.bfloat16)
    )(*directions, gate_in)
    across = (((1,), (1,)), ((), ()))
    partial_value = lax.dot_general(
        hidden, mixer[:, 2 * channels :], across, preferred_element_type=jnp.float32
    )
    share = tokens.shape[0] // lax.axis_size(TP)
    place = lax.axis_index("c") * lax.axis_size("x") + lax.axis_index("x")
    own = lax.dynamic_slice_in_dim(tokens, place * share, share, axis=0)
    own, partial_value, mixer_gain, norm_gain, out_gain = lax.optimization_barrier(
        (
            own,
            partial_value.astype(jnp.bfloat16),
            recurrent_output_gain.astype(jnp.float32),
            feedforward_norm_gain.astype(jnp.float32),
            feedforward_output_gain.astype(jnp.float32),
        )
    )
    mixed = summed_rows(partial_value)
    stream = lax.optimization_barrier(
        (own.astype(jnp.float32) + root_norm(mixed, mixer_gain)).astype(jnp.bfloat16)
    )
    normed_ff = all_rows(
        root_norm(stream.astype(jnp.float32), norm_gain).astype(jnp.bfloat16)
    )
    lifted_sum = jnp.dot(normed_ff, forward[:, :hidden_units], preferred_element_type=jnp.float32)
    lifted = jnp.square(jax.nn.relu(lifted_sum)).astype(jnp.bfloat16)
    lowered_part = lax.dot_general(
        lifted, forward[:, hidden_units:], across, preferred_element_type=jnp.float32
    )
    lowered = summed_rows(lowered_part)
    return all_rows(
        (stream.astype(jnp.float32) + root_norm(lowered, out_gain)).astype(
            jnp.bfloat16
        )
    )


def solution(mesh):
    split = Mesh(mesh.devices.reshape(4, 4, 4, 4, 2), ("zh", "zl", "y", "x", "c"))
    placed = (
        P(FS, None),
        P(),
        P(FS, TP),
        P(FS, TP),
        P(None, TP),
        P(None, TP, None, None),
        P(None, TP, None, None),
        P(None, TP),
        P(None, FS, TP),
        P(TP, FS),
        P(),
        P(),
        P(FS, TP),
        P(TP, FS),
        P(),
    )
    return jax.shard_map(
        per_device, mesh=split, in_specs=placed, out_specs=P(FS, None), check_vma=False
    )
```

```python
import jax
import jax.numpy as jnp
from jax import lax
from jax.experimental import pallas as pl
from jax.experimental.pallas import tpu as pltpu
from jax.sharding import Mesh
from jax.sharding import PartitionSpec as P

FS = ("zh", "zl", "y")
Z = ("zh", "zl")
TP = ("x", "c")


EPS = 1e-06
GATE_STEEPNESS = 8.0


def spread(array, axis):
    copies = jnp.broadcast_to(array, (lax.axis_size(axis), *array.shape))
    return lax.all_to_all(copies, axis, split_axis=0, concat_axis=0, tiled=True)


def mixer_weights(array):
    rows, width = array.shape
    pieces = spread(lax.all_gather(array, Z, axis=0, tiled=True), "y")
    pieces = pieces.reshape(pieces.shape[0], -1, rows, width)
    return jnp.transpose(pieces, (1, 0, 2, 3)).reshape(-1, width)


def feedforward_weights(array):
    near = spread(array, "y").reshape(-1, array.shape[-1])
    return lax.all_gather(near, Z, axis=0, tiled=True)


def summed_rows(partial):
    cores, wide = lax.axis_size("c"), lax.axis_size("x")
    rows, width = partial.shape
    halves = partial.astype(jnp.bfloat16).reshape(cores, rows // cores, width)
    pair = lax.all_to_all(halves, "c", split_axis=0, concat_axis=0, tiled=True)
    half = jnp.sum(pair.astype(jnp.float32), axis=0).astype(jnp.bfloat16)
    quarters = half.reshape(wide, rows // (cores * wide), width)
    several = lax.all_to_all(quarters, "x", split_axis=0, concat_axis=0, tiled=True)
    return jnp.sum(several.astype(jnp.float32), axis=0)


def all_rows(part):
    return spread(spread(part, "x"), "c").reshape(-1, part.shape[-1])


def root_norm(values, gain):
    return (
        values
        * lax.rsqrt(jnp.mean(values * values, axis=-1, keepdims=True) + EPS)
        * gain.astype(jnp.float32)
    )


def swept(decay, drive, backward):
    length = decay.shape[0]
    place = lax.broadcasted_iota(jnp.int32, decay.shape, 0)
    step = 1
    while step < length:
        if step % 8:
            turn = length - step if backward else step
            inside = place < length - step if backward else place >= step
            far_decay = jnp.where(inside, pltpu.roll(decay, turn, 0), 1.0)
            far_drive = jnp.where(inside, pltpu.roll(drive, turn, 0), 0.0)
        else:
            one = jnp.ones((step, decay.shape[1]), jnp.float32)
            if backward:
                far_decay = jnp.concatenate((decay[step:], one), axis=0)
                far_drive = jnp.concatenate((drive[step:], 0.0 * one), axis=0)
            else:
                far_decay = jnp.concatenate((one, decay[:-step]), axis=0)
                far_drive = jnp.concatenate((0.0 * one, drive[:-step]), axis=0)
        drive = drive + decay * far_drive
        decay = decay * far_decay
        step *= 2
    return drive


def shifted(values, by):
    if by == 0:
        return values
    length = values.shape[0]
    place = lax.broadcasted_iota(jnp.int32, values.shape, 0)
    inside = place >= by if by > 0 else place < length + by
    return jnp.where(inside, pltpu.roll(values, by % length, 0), 0.0)


def one_less_exp(x):
    series = jnp.ones(x.shape, jnp.float32)
    for degree in range(8, 1, -1):
        series = 1.0 + x * series * (1.0 / degree)
    return jnp.where(jnp.abs(x) < 0.4, -x * series, 1.0 - jnp.exp(x))


def hidden_kernel(both, taps, retention, admission, rate, extra, out):
    channels = out.shape[1]
    signal = both[:, :channels].astype(jnp.float32)
    width_taps = taps.shape[0]
    total = jnp.zeros(signal.shape, jnp.float32)
    for offset in range(width_taps):
        total = total + shifted(signal, width_taps // 2 - offset) * taps[offset : offset + 1, :]
    conv_out = total.astype(jnp.bfloat16)
    wide = conv_out.astype(jnp.float32)
    state = jnp.zeros(signal.shape, jnp.float32)
    for way in range(2):
        retain = jax.nn.sigmoid(
            jnp.dot(conv_out, retention[way], preferred_element_type=jnp.float32)
        )
        admit = jax.nn.sigmoid(
            jnp.dot(conv_out, admission[way], preferred_element_type=jnp.float32)
        )
        log_decay = -GATE_STEEPNESS * retain * rate[way : way + 1, :] + extra[way]
        drive = jnp.sqrt(one_less_exp(2.0 * log_decay)) * (admit * wide)
        state = state + swept(jnp.exp(log_decay), drive, way == 1)
    out[...] = (state * jax.nn.gelu(both[:, channels:].astype(jnp.float32))).astype(out.dtype)


def per_device(
    tokens,
    recurrent_input_gain,
    recurrent_branch_weight,
    output_gate_weight,
    filter_taps,
    retention_gate_blocks,
    input_gate_blocks,
    channel_decay_rate,
    position_log_decay,
    recurrent_output_weight,
    recurrent_output_gain,
    feedforward_norm_gain,
    feedforward_up_weight,
    feedforward_down_weight,
    feedforward_output_gain,
):
    channels = recurrent_branch_weight.shape[1]
    hidden_units = feedforward_up_weight.shape[1]
    early = hidden_units - channels
    down_rows = feedforward_down_weight.T
    mixer = mixer_weights(
        jnp.concatenate(
            (
                recurrent_branch_weight,
                output_gate_weight,
                recurrent_output_weight.T,
                down_rows[:, early:],
            ),
            axis=1,
        )
    )
    forward = feedforward_weights(
        jnp.concatenate((feedforward_up_weight, down_rows[:, :early]), axis=1)
    )
    normed = root_norm(tokens.astype(jnp.float32), recurrent_input_gain).astype(jnp.bfloat16)
    both = jnp.dot(
        normed, mixer[:, : 2 * channels], preferred_element_type=jnp.float32
    ).astype(jnp.bfloat16)
    hidden = pl.pallas_call(
        hidden_kernel, out_shape=jax.ShapeDtypeStruct((both.shape[0], channels), jnp.bfloat16)
    )(
        both,
        filter_taps.astype(jnp.float32),
        retention_gate_blocks.reshape(2, channels, channels),
        input_gate_blocks.reshape(2, channels, channels),
        channel_decay_rate,
        position_log_decay,
    )
    across = (((1,), (1,)), ((), ()))
    partial_value = lax.dot_general(
        hidden, mixer[:, 2 * channels : 3 * channels], across, preferred_element_type=jnp.float32
    )
    share = tokens.shape[0] // lax.axis_size(TP)
    place = lax.axis_index("c") * lax.axis_size("x") + lax.axis_index("x")
    own = lax.dynamic_slice_in_dim(tokens, place * share, share, axis=0)
    own, partial_value, mixer_gain, norm_gain, out_gain = lax.optimization_barrier(
        (
            own,
            partial_value.astype(jnp.bfloat16),
            recurrent_output_gain.astype(jnp.float32),
            feedforward_norm_gain.astype(jnp.float32),
            feedforward_output_gain.astype(jnp.float32),
        )
    )
    mixed = summed_rows(partial_value)
    stream = lax.optimization_barrier(
        (own.astype(jnp.float32) + root_norm(mixed, mixer_gain)).astype(jnp.bfloat16)
    )
    normed_ff = all_rows(
        root_norm(stream.astype(jnp.float32), norm_gain).astype(jnp.bfloat16)
    )
    lifted_sum = jnp.dot(normed_ff, forward[:, :hidden_units], preferred_element_type=jnp.float32)
    lifted = jnp.square(jax.nn.relu(lifted_sum)).astype(jnp.bfloat16)
    lowered_part = lax.dot_general(
        lifted[:, :early], forward[:, hidden_units:], across, preferred_element_type=jnp.float32
    ) + lax.dot_general(
        lifted[:, early:], mixer[:, 3 * channels :], across, preferred_element_type=jnp.float32
    )
    lowered = summed_rows(lowered_part)
    return all_rows(
        (stream.astype(jnp.float32) + root_norm(lowered, out_gain)).astype(
            jnp.bfloat16
        )
    )


def solution(mesh):
    split = Mesh(mesh.devices.reshape(4, 4, 4, 4, 2), ("zh", "zl", "y", "x", "c"))
    placed = (
        P(FS, None),
        P(),
        P(FS, TP),
        P(FS, TP),
        P(None, TP),
        P(None, TP, None, None),
        P(None, TP, None, None),
        P(None, TP),
        P(None, FS, TP),
        P(TP, FS),
        P(),
        P(),
        P(FS, TP),
        P(TP, FS),
        P(),
    )
    return jax.shard_map(
        per_device, mesh=split, in_specs=placed, out_specs=P(FS, None), check_vma=False
    )
```

```python
import jax
import jax.numpy as jnp
from jax import lax
from jax.experimental import pallas as pl
from jax.experimental.pallas import tpu as pltpu
from jax.sharding import Mesh
from jax.sharding import PartitionSpec as P

FS = ("zh", "zl", "y")
Z = ("zh", "zl")
TP = ("x", "c")


EPS = 1e-06
GATE_STEEPNESS = 8.0


def spread(array, axis):
    copies = jnp.broadcast_to(array, (lax.axis_size(axis), *array.shape))
    return lax.all_to_all(copies, axis, split_axis=0, concat_axis=0, tiled=True)


def in_order(pieces, rows):
    width = pieces.shape[-1]
    pieces = pieces.reshape(pieces.shape[0], -1, rows, width)
    return jnp.transpose(pieces, (1, 0, 2, 3)).reshape(-1, width)


def sent_round(array, axis):
    size = lax.axis_size(axis)
    pieces = [array]
    for step in range(1, size):
        ring = [(i, (i + step) % size) for i in range(size)]
        pieces.append(lax.ppermute(array, axis, ring))
    return pieces


def set_in_order(pieces, axis, rows):
    size, here = lax.axis_size(axis), lax.axis_index(axis)
    deep, width = pieces[0].shape[0] // rows, pieces[0].shape[1]
    out = jnp.zeros((deep, size, rows, width), pieces[0].dtype)
    for step, piece in enumerate(pieces):
        block = piece.reshape(deep, 1, rows, width)
        out = lax.dynamic_update_slice(out, block, (0, (here - step) % size, 0, 0))
    return out.reshape(-1, width)


def feedforward_weights(array):
    near = spread(array, "y").reshape(-1, array.shape[-1])
    return lax.all_gather(near, Z, axis=0, tiled=True)


def summed_rows(partial):
    cores, wide = lax.axis_size("c"), lax.axis_size("x")
    rows, width = partial.shape
    halves = partial.astype(jnp.bfloat16).reshape(cores, rows // cores, width)
    pair = lax.all_to_all(halves, "c", split_axis=0, concat_axis=0, tiled=True)
    half = jnp.sum(pair.astype(jnp.float32), axis=0).astype(jnp.bfloat16)
    quarters = half.reshape(wide, rows // (cores * wide), width)
    several = lax.all_to_all(quarters, "x", split_axis=0, concat_axis=0, tiled=True)
    return jnp.sum(several.astype(jnp.float32), axis=0)


def all_rows(part):
    return spread(spread(part, "x"), "c").reshape(-1, part.shape[-1])


def root_norm(values, gain):
    return (
        values
        * lax.rsqrt(jnp.mean(values * values, axis=-1, keepdims=True) + EPS)
        * gain.astype(jnp.float32)
    )


def swept(decay, drive, backward):
    length = decay.shape[0]
    place = lax.broadcasted_iota(jnp.int32, decay.shape, 0)
    step = 1
    while step < length:
        if step % 8:
            turn = length - step if backward else step
            inside = place < length - step if backward else place >= step
            far_decay = jnp.where(inside, pltpu.roll(decay, turn, 0), 1.0)
            far_drive = jnp.where(inside, pltpu.roll(drive, turn, 0), 0.0)
        else:
            one = jnp.ones((step, decay.shape[1]), jnp.float32)
            if backward:
                far_decay = jnp.concatenate((decay[step:], one), axis=0)
                far_drive = jnp.concatenate((drive[step:], 0.0 * one), axis=0)
            else:
                far_decay = jnp.concatenate((one, decay[:-step]), axis=0)
                far_drive = jnp.concatenate((0.0 * one, drive[:-step]), axis=0)
        drive = drive + decay * far_drive
        decay = decay * far_decay
        step *= 2
    return drive


def shifted(values, by):
    if by == 0:
        return values
    length = values.shape[0]
    place = lax.broadcasted_iota(jnp.int32, values.shape, 0)
    inside = place >= by if by > 0 else place < length + by
    return jnp.where(inside, pltpu.roll(values, by % length, 0), 0.0)


def one_less_exp(x):
    series = jnp.ones(x.shape, jnp.float32)
    for degree in range(8, 1, -1):
        series = 1.0 + x * series * (1.0 / degree)
    return jnp.where(jnp.abs(x) < 0.4, -x * series, 1.0 - jnp.exp(x))


def hidden_kernel(both, taps, retention, admission, rate, extra, out):
    channels = out.shape[1]
    signal = both[:, :channels].astype(jnp.float32)
    width_taps = taps.shape[0]
    total = jnp.zeros(signal.shape, jnp.float32)
    for offset in range(width_taps):
        total = total + shifted(signal, width_taps // 2 - offset) * taps[offset : offset + 1, :]
    conv_out = total.astype(jnp.bfloat16)
    wide = conv_out.astype(jnp.float32)
    state = jnp.zeros(signal.shape, jnp.float32)
    for way in range(2):
        retain = jax.nn.sigmoid(
            jnp.dot(conv_out, retention[way], preferred_element_type=jnp.float32)
        )
        admit = jax.nn.sigmoid(
            jnp.dot(conv_out, admission[way], preferred_element_type=jnp.float32)
        )
        log_decay = -GATE_STEEPNESS * retain * rate[way : way + 1, :] + extra[way]
        drive = jnp.sqrt(one_less_exp(2.0 * log_decay)) * (admit * wide)
        state = state + swept(jnp.exp(log_decay), drive, way == 1)
    out[...] = (state * jax.nn.gelu(both[:, channels:].astype(jnp.float32))).astype(out.dtype)


def per_device(
    tokens,
    recurrent_input_gain,
    recurrent_branch_weight,
    output_gate_weight,
    filter_taps,
    retention_gate_blocks,
    input_gate_blocks,
    channel_decay_rate,
    position_log_decay,
    recurrent_output_weight,
    recurrent_output_gain,
    feedforward_norm_gain,
    feedforward_up_weight,
    feedforward_down_weight,
    feedforward_output_gain,
):
    channels = recurrent_branch_weight.shape[1]
    hidden_units = feedforward_up_weight.shape[1]
    rows = recurrent_branch_weight.shape[0]
    early = hidden_units - 2 * channels
    forward = feedforward_weights(
        jnp.concatenate((feedforward_up_weight[:, :early], feedforward_down_weight.T), axis=1)
    )
    column = lax.all_gather(
        jnp.concatenate(
            (
                recurrent_branch_weight,
                output_gate_weight,
                recurrent_output_weight.T,
                feedforward_up_weight[:, early:],
            ),
            axis=1,
        ),
        Z,
        axis=0,
        tiled=True,
    )
    mixer = spread(column[:, : 3 * channels], "y")
    late, mixer = lax.optimization_barrier((column[:, 3 * channels :], mixer))
    late = sent_round(late, "y")
    mixer = in_order(mixer, rows)
    normed = root_norm(tokens.astype(jnp.float32), recurrent_input_gain).astype(jnp.bfloat16)
    both = jnp.dot(
        normed, mixer[:, : 2 * channels], preferred_element_type=jnp.float32
    ).astype(jnp.bfloat16)
    hidden = pl.pallas_call(
        hidden_kernel, out_shape=jax.ShapeDtypeStruct((both.shape[0], channels), jnp.bfloat16)
    )(
        both,
        filter_taps.astype(jnp.float32),
        retention_gate_blocks.reshape(2, channels, channels),
        input_gate_blocks.reshape(2, channels, channels),
        channel_decay_rate,
        position_log_decay,
    )
    across = (((1,), (1,)), ((), ()))
    partial_value = lax.dot_general(
        hidden, mixer[:, 2 * channels :], across, preferred_element_type=jnp.float32
    )
    share = tokens.shape[0] // lax.axis_size(TP)
    place = lax.axis_index("c") * lax.axis_size("x") + lax.axis_index("x")
    own = lax.dynamic_slice_in_dim(tokens, place * share, share, axis=0)
    own, partial_value, mixer_gain, norm_gain, out_gain = lax.optimization_barrier(
        (
            own,
            partial_value.astype(jnp.bfloat16),
            recurrent_output_gain.astype(jnp.float32),
            feedforward_norm_gain.astype(jnp.float32),
            feedforward_output_gain.astype(jnp.float32),
        )
    )
    mixed = summed_rows(partial_value)
    stream = lax.optimization_barrier(
        (own.astype(jnp.float32) + root_norm(mixed, mixer_gain)).astype(jnp.bfloat16)
    )
    normed_ff = all_rows(
        root_norm(stream.astype(jnp.float32), norm_gain).astype(jnp.bfloat16)
    )
    late, normed_ff = lax.optimization_barrier((late, normed_ff))
    lifted = [
        jnp.square(
            jax.nn.relu(jnp.dot(normed_ff, weight, preferred_element_type=jnp.float32))
        ).astype(jnp.bfloat16)
        for weight in (forward[:, :early], set_in_order(late, "y", rows))
    ]
    lowered_part = lax.dot_general(
        jnp.concatenate(lifted, axis=1), forward[:, early:], across, preferred_element_type=jnp.float32
    )
    lowered = summed_rows(lowered_part)
    return all_rows(
        (stream.astype(jnp.float32) + root_norm(lowered, out_gain)).astype(
            jnp.bfloat16
        )
    )


def solution(mesh):
    split = Mesh(mesh.devices.reshape(4, 4, 4, 4, 2), ("zh", "zl", "y", "x", "c"))
    placed = (
        P(FS, None),
        P(),
        P(FS, TP),
        P(FS, TP),
        P(None, TP),
        P(None, TP, None, None),
        P(None, TP, None, None),
        P(None, TP),
        P(None, FS, TP),
        P(TP, FS),
        P(),
        P(),
        P(FS, TP),
        P(TP, FS),
        P(),
    )
    return jax.shard_map(
        per_device, mesh=split, in_specs=placed, out_specs=P(FS, None), check_vma=False
    )
```

```python
import jax
import jax.numpy as jnp
from jax import lax
from jax.experimental import pallas as pl
from jax.experimental.pallas import tpu as pltpu
from jax.sharding import Mesh
from jax.sharding import PartitionSpec as P

FS = ("zh", "zl", "y")
Z = ("zh", "zl")
TP = ("x", "c")


EPS = 1e-06
GATE_STEEPNESS = 8.0


def spread(array, axis):
    copies = jnp.broadcast_to(array, (lax.axis_size(axis), *array.shape))
    return lax.all_to_all(copies, axis, split_axis=0, concat_axis=0, tiled=True)


def in_order(pieces, rows):
    width = pieces.shape[-1]
    pieces = pieces.reshape(pieces.shape[0], -1, rows, width)
    return jnp.transpose(pieces, (1, 0, 2, 3)).reshape(-1, width)


def sent_round(array, axis):
    size = lax.axis_size(axis)
    pieces = [array]
    for step in range(1, size):
        ring = [(i, (i + step) % size) for i in range(size)]
        pieces.append(lax.ppermute(array, axis, ring))
    return pieces


def set_in_order(pieces, places, rows):
    size = len(pieces)
    deep, width = pieces[0].shape[0] // rows, pieces[0].shape[1]
    out = jnp.zeros((deep, size, rows, width), pieces[0].dtype)
    nought = jnp.uint32(0)
    for place, piece in zip(places, pieces):
        block = piece.reshape(deep, 1, rows, width)
        out = lax.dynamic_update_slice(out, block, (nought, place, nought, nought))
    return out.reshape(-1, width)


def feedforward_weights(array):
    near = spread(array, "y").reshape(-1, array.shape[-1])
    return lax.all_gather(near, Z, axis=0, tiled=True)


def summed_rows(partial):
    cores, wide = lax.axis_size("c"), lax.axis_size("x")
    rows, width = partial.shape
    halves = partial.astype(jnp.bfloat16).reshape(cores, rows // cores, width)
    pair = lax.all_to_all(halves, "c", split_axis=0, concat_axis=0, tiled=True)
    half = jnp.sum(pair.astype(jnp.float32), axis=0).astype(jnp.bfloat16)
    quarters = half.reshape(wide, rows // (cores * wide), width)
    several = lax.all_to_all(quarters, "x", split_axis=0, concat_axis=0, tiled=True)
    return jnp.sum(several.astype(jnp.float32), axis=0)


def all_rows(part):
    return spread(spread(part, "x"), "c").reshape(-1, part.shape[-1])


def root_norm(values, gain):
    return (
        values
        * lax.rsqrt(jnp.mean(values * values, axis=-1, keepdims=True) + EPS)
        * gain.astype(jnp.float32)
    )


def swept(decay, drive, backward):
    length = decay.shape[0]
    place = lax.broadcasted_iota(jnp.int32, decay.shape, 0)
    step = 1
    while step < length:
        if step % 8:
            turn = length - step if backward else step
            inside = place < length - step if backward else place >= step
            far_decay = jnp.where(inside, pltpu.roll(decay, turn, 0), 1.0)
            far_drive = jnp.where(inside, pltpu.roll(drive, turn, 0), 0.0)
        else:
            one = jnp.ones((step, decay.shape[1]), jnp.float32)
            if backward:
                far_decay = jnp.concatenate((decay[step:], one), axis=0)
                far_drive = jnp.concatenate((drive[step:], 0.0 * one), axis=0)
            else:
                far_decay = jnp.concatenate((one, decay[:-step]), axis=0)
                far_drive = jnp.concatenate((0.0 * one, drive[:-step]), axis=0)
        drive = drive + decay * far_drive
        decay = decay * far_decay
        step *= 2
    return drive


def shifted(values, by):
    if by == 0:
        return values
    length = values.shape[0]
    place = lax.broadcasted_iota(jnp.int32, values.shape, 0)
    inside = place >= by if by > 0 else place < length + by
    return jnp.where(inside, pltpu.roll(values, by % length, 0), 0.0)


def one_less_exp(x):
    series = jnp.ones(x.shape, jnp.float32)
    for degree in range(8, 1, -1):
        series = 1.0 + x * series * (1.0 / degree)
    return jnp.where(jnp.abs(x) < 0.4, -x * series, 1.0 - jnp.exp(x))


def hidden_kernel(both, taps, retention, admission, rate, extra, out):
    channels = out.shape[1]
    signal = both[:, :channels].astype(jnp.float32)
    width_taps = taps.shape[0]
    total = jnp.zeros(signal.shape, jnp.float32)
    for offset in range(width_taps):
        total = total + shifted(signal, width_taps // 2 - offset) * taps[offset : offset + 1, :]
    conv_out = total.astype(jnp.bfloat16)
    wide = conv_out.astype(jnp.float32)
    state = jnp.zeros(signal.shape, jnp.float32)
    for way in range(2):
        retain = jax.nn.sigmoid(
            jnp.dot(conv_out, retention[way], preferred_element_type=jnp.float32)
        )
        admit = jax.nn.sigmoid(
            jnp.dot(conv_out, admission[way], preferred_element_type=jnp.float32)
        )
        log_decay = -GATE_STEEPNESS * retain * rate[way : way + 1, :] + extra[way]
        drive = jnp.sqrt(one_less_exp(2.0 * log_decay)) * (admit * wide)
        state = state + swept(jnp.exp(log_decay), drive, way == 1)
    out[...] = (state * jax.nn.gelu(both[:, channels:].astype(jnp.float32))).astype(out.dtype)


def per_device(
    tokens,
    recurrent_input_gain,
    recurrent_branch_weight,
    output_gate_weight,
    filter_taps,
    retention_gate_blocks,
    input_gate_blocks,
    channel_decay_rate,
    position_log_decay,
    recurrent_output_weight,
    recurrent_output_gain,
    feedforward_norm_gain,
    feedforward_up_weight,
    feedforward_down_weight,
    feedforward_output_gain,
):
    channels = recurrent_branch_weight.shape[1]
    hidden_units = feedforward_up_weight.shape[1]
    rows = recurrent_branch_weight.shape[0]
    early = hidden_units - 2 * channels
    forward = feedforward_weights(
        jnp.concatenate((feedforward_up_weight[:, :early], feedforward_down_weight.T), axis=1)
    )
    column = lax.all_gather(
        jnp.concatenate(
            (
                recurrent_branch_weight,
                output_gate_weight,
                recurrent_output_weight.T,
                feedforward_up_weight[:, early:],
            ),
            axis=1,
        ),
        Z,
        axis=0,
        tiled=True,
    )
    mixer = spread(column[:, : 3 * channels], "y")
    late, mixer = lax.optimization_barrier((column[:, 3 * channels :], mixer))
    late = sent_round(late, "y")
    mixer = in_order(mixer, rows)
    normed = lax.optimization_barrier(
        root_norm(tokens.astype(jnp.float32), recurrent_input_gain).astype(jnp.bfloat16)
    )
    both = jnp.dot(
        normed, mixer[:, : 2 * channels], preferred_element_type=jnp.float32
    ).astype(jnp.bfloat16)
    hidden = pl.pallas_call(
        hidden_kernel, out_shape=jax.ShapeDtypeStruct((both.shape[0], channels), jnp.bfloat16)
    )(
        both,
        filter_taps.astype(jnp.float32),
        retention_gate_blocks.reshape(2, channels, channels),
        input_gate_blocks.reshape(2, channels, channels),
        channel_decay_rate,
        position_log_decay,
    )
    across = (((1,), (1,)), ((), ()))
    partial_value = lax.dot_general(
        hidden, mixer[:, 2 * channels :], across, preferred_element_type=jnp.float32
    )
    share = tokens.shape[0] // lax.axis_size(TP)
    place = lax.axis_index("c") * lax.axis_size("x") + lax.axis_index("x")
    own = lax.dynamic_slice_in_dim(tokens, place * share, share, axis=0)
    span = lax.axis_size("y")
    turn = lax.axis_index("y").astype(jnp.uint32)
    places = [(turn + (span - step)) % span for step in range(span)]
    places, own, partial_value, mixer_gain, norm_gain, out_gain = lax.optimization_barrier(
        (
            places,
            own,
            partial_value.astype(jnp.bfloat16),
            recurrent_output_gain.astype(jnp.float32),
            feedforward_norm_gain.astype(jnp.float32),
            feedforward_output_gain.astype(jnp.float32),
        )
    )
    mixed = summed_rows(partial_value)
    stream = lax.optimization_barrier(
        (own.astype(jnp.float32) + root_norm(mixed, mixer_gain)).astype(jnp.bfloat16)
    )
    half = spread(root_norm(stream.astype(jnp.float32), norm_gain).astype(jnp.bfloat16), "x")
    half = lax.optimization_barrier(half)
    normed_ff = spread(half, "c").reshape(tokens.shape)
    lifted = [
        jnp.square(
            jax.nn.relu(jnp.dot(normed_ff, weight, preferred_element_type=jnp.float32))
        ).astype(jnp.bfloat16)
        for weight in (forward[:, :early], set_in_order(late, places, rows))
    ]
    lowered_part = lax.dot_general(
        jnp.concatenate(lifted, axis=1), forward[:, early:], across, preferred_element_type=jnp.float32
    )
    lowered = summed_rows(lowered_part)
    return all_rows(
        (stream.astype(jnp.float32) + root_norm(lowered, out_gain)).astype(
            jnp.bfloat16
        )
    )


def solution(mesh):
    split = Mesh(mesh.devices.reshape(4, 4, 4, 4, 2), ("zh", "zl", "y", "x", "c"))
    placed = (
        P(FS, None),
        P(),
        P(FS, TP),
        P(FS, TP),
        P(None, TP),
        P(None, TP, None, None),
        P(None, TP, None, None),
        P(None, TP),
        P(None, FS, TP),
        P(TP, FS),
        P(),
        P(),
        P(FS, TP),
        P(TP, FS),
        P(),
    )
    return jax.shard_map(
        per_device, mesh=split, in_specs=placed, out_specs=P(FS, None), check_vma=False
    )
```

```python
import jax
import jax.numpy as jnp
from jax import lax
from jax.experimental import pallas as pl
from jax.experimental.pallas import tpu as pltpu
from jax.sharding import Mesh
from jax.sharding import PartitionSpec as P

FS = ("zh", "zl", "y")
Z = ("zh", "zl")
TP = ("x", "c")


EPS = 1e-06
GATE_STEEPNESS = 8.0


def spread(array, axis):
    copies = jnp.broadcast_to(array, (lax.axis_size(axis), *array.shape))
    return lax.all_to_all(copies, axis, split_axis=0, concat_axis=0, tiled=True)


def in_order(pieces, rows):
    width = pieces.shape[-1]
    pieces = pieces.reshape(pieces.shape[0], -1, rows, width)
    return jnp.transpose(pieces, (1, 0, 2, 3)).reshape(-1, width)


def sent_round(array, axis):
    size = lax.axis_size(axis)
    pieces = [array]
    for step in range(1, size):
        ring = [(i, (i + step) % size) for i in range(size)]
        pieces.append(lax.ppermute(array, axis, ring))
    return pieces


def set_in(out, piece, place):
    deep, _, rows, width = out.shape
    nought = jnp.uint32(0)
    block = piece.reshape(deep, 1, rows, width)
    return lax.dynamic_update_slice(out, block, (nought, place, nought, nought))


def feedforward_weights(array):
    near = spread(array, "y").reshape(-1, array.shape[-1])
    return lax.all_gather(near, Z, axis=0, tiled=True)


def summed_rows(partial):
    cores, wide = lax.axis_size("c"), lax.axis_size("x")
    rows, width = partial.shape
    halves = partial.astype(jnp.bfloat16).reshape(cores, rows // cores, width)
    pair = lax.all_to_all(halves, "c", split_axis=0, concat_axis=0, tiled=True)
    half = jnp.sum(pair.astype(jnp.float32), axis=0).astype(jnp.bfloat16)
    quarters = half.reshape(wide, rows // (cores * wide), width)
    several = lax.all_to_all(quarters, "x", split_axis=0, concat_axis=0, tiled=True)
    return jnp.sum(several.astype(jnp.float32), axis=0)


def all_rows(part):
    half = spread(part, "x").reshape(-1, part.shape[-1])
    other = lax.ppermute(half, "c", [(0, 1), (1, 0)])
    mine = lax.broadcasted_iota(jnp.int32, (2, 1, 1), 0) == lax.axis_index("c")
    return jnp.where(mine, half[None], other[None]).reshape(-1, part.shape[-1])


def root_norm(values, gain):
    return (
        values
        * lax.rsqrt(jnp.mean(values * values, axis=-1, keepdims=True) + EPS)
        * gain.astype(jnp.float32)
    )


def swept(decay, drive, backward):
    length = decay.shape[0]
    place = lax.broadcasted_iota(jnp.int32, decay.shape, 0)
    step = 1
    while step < length:
        if step % 8:
            turn = length - step if backward else step
            inside = place < length - step if backward else place >= step
            far_decay = jnp.where(inside, pltpu.roll(decay, turn, 0), 1.0)
            far_drive = jnp.where(inside, pltpu.roll(drive, turn, 0), 0.0)
        else:
            one = jnp.ones((step, decay.shape[1]), jnp.float32)
            if backward:
                far_decay = jnp.concatenate((decay[step:], one), axis=0)
                far_drive = jnp.concatenate((drive[step:], 0.0 * one), axis=0)
            else:
                far_decay = jnp.concatenate((one, decay[:-step]), axis=0)
                far_drive = jnp.concatenate((0.0 * one, drive[:-step]), axis=0)
        drive = drive + decay * far_drive
        decay = decay * far_decay
        step *= 2
    return drive


def shifted(values, by):
    if by == 0:
        return values
    length = values.shape[0]
    place = lax.broadcasted_iota(jnp.int32, values.shape, 0)
    inside = place >= by if by > 0 else place < length + by
    return jnp.where(inside, pltpu.roll(values, by % length, 0), 0.0)


def one_less_exp(x):
    series = jnp.ones(x.shape, jnp.float32)
    for degree in range(8, 1, -1):
        series = 1.0 + x * series * (1.0 / degree)
    return jnp.where(jnp.abs(x) < 0.4, -x * series, 1.0 - jnp.exp(x))


def hidden_kernel(both, taps, retention, admission, rate, extra, out):
    channels = out.shape[1]
    signal = both[:, :channels].astype(jnp.float32)
    width_taps = taps.shape[0]
    total = jnp.zeros(signal.shape, jnp.float32)
    for offset in range(width_taps):
        total = total + shifted(signal, width_taps // 2 - offset) * taps[offset : offset + 1, :]
    conv_out = total.astype(jnp.bfloat16)
    wide = conv_out.astype(jnp.float32)
    state = jnp.zeros(signal.shape, jnp.float32)
    for way in range(2):
        retain = jax.nn.sigmoid(
            jnp.dot(conv_out, retention[way], preferred_element_type=jnp.float32)
        )
        admit = jax.nn.sigmoid(
            jnp.dot(conv_out, admission[way], preferred_element_type=jnp.float32)
        )
        log_decay = -GATE_STEEPNESS * retain * rate[way : way + 1, :] + extra[way]
        drive = jnp.sqrt(one_less_exp(2.0 * log_decay)) * (admit * wide)
        state = state + swept(jnp.exp(log_decay), drive, way == 1)
    out[...] = (state * jax.nn.gelu(both[:, channels:].astype(jnp.float32))).astype(out.dtype)


def per_device(
    tokens,
    recurrent_input_gain,
    recurrent_branch_weight,
    output_gate_weight,
    filter_taps,
    retention_gate_blocks,
    input_gate_blocks,
    channel_decay_rate,
    position_log_decay,
    recurrent_output_weight,
    recurrent_output_gain,
    feedforward_norm_gain,
    feedforward_up_weight,
    feedforward_down_weight,
    feedforward_output_gain,
):
    channels = recurrent_branch_weight.shape[1]
    hidden_units = feedforward_up_weight.shape[1]
    rows = recurrent_branch_weight.shape[0]
    early = hidden_units - channels
    forward = feedforward_weights(
        jnp.concatenate((feedforward_up_weight[:, :early], feedforward_down_weight.T), axis=1)
    )
    column = lax.all_gather(
        jnp.concatenate(
            (
                recurrent_branch_weight,
                output_gate_weight,
                recurrent_output_weight.T,
                feedforward_up_weight[:, early:],
            ),
            axis=1,
        ),
        Z,
        axis=0,
        tiled=True,
    )
    mixer = spread(column[:, : 3 * channels], "y")
    late, mixer = lax.optimization_barrier((column[:, 3 * channels :], mixer))
    late = sent_round(late, "y")
    mixer = in_order(mixer, rows)
    normed = lax.optimization_barrier(
        root_norm(tokens.astype(jnp.float32), recurrent_input_gain).astype(jnp.bfloat16)
    )
    both = jnp.dot(
        normed, mixer[:, : 2 * channels], preferred_element_type=jnp.float32
    ).astype(jnp.bfloat16)
    hidden = pl.pallas_call(
        hidden_kernel, out_shape=jax.ShapeDtypeStruct((both.shape[0], channels), jnp.bfloat16)
    )(
        both,
        filter_taps.astype(jnp.float32),
        retention_gate_blocks.reshape(2, channels, channels),
        input_gate_blocks.reshape(2, channels, channels),
        channel_decay_rate,
        position_log_decay,
    )
    across = (((1,), (1,)), ((), ()))
    partial_value = lax.dot_general(
        hidden, mixer[:, 2 * channels :], across, preferred_element_type=jnp.float32
    )
    share = tokens.shape[0] // lax.axis_size(TP)
    place = lax.axis_index("c") * lax.axis_size("x") + lax.axis_index("x")
    own = lax.dynamic_slice_in_dim(tokens, place * share, share, axis=0)
    span = lax.axis_size("y")
    turn = lax.axis_index("y").astype(jnp.uint32)
    places = [(turn + (span - step)) % span for step in range(span)]
    late_width = late[0].shape[1]
    late_up = jnp.zeros((late[0].shape[0] // rows, span, rows, late_width), jnp.bfloat16)
    late_up = set_in(late_up, late[0], places[0])
    late_up, places, own, partial_value, mixer_gain, norm_gain, out_gain = lax.optimization_barrier(
        (
            late_up,
            places,
            own,
            partial_value.astype(jnp.bfloat16),
            recurrent_output_gain.astype(jnp.float32),
            feedforward_norm_gain.astype(jnp.float32),
            feedforward_output_gain.astype(jnp.float32),
        )
    )
    mixed = summed_rows(partial_value)
    stream = lax.optimization_barrier(
        (own.astype(jnp.float32) + root_norm(mixed, mixer_gain)).astype(jnp.bfloat16)
    )
    half = spread(root_norm(stream.astype(jnp.float32), norm_gain).astype(jnp.bfloat16), "x")
    half = lax.optimization_barrier(half)
    normed_ff = spread(half, "c").reshape(tokens.shape)
    for piece, spot in zip(late[1:], places[1:]):
        late_up = set_in(late_up, piece, spot)
    lifted = [
        jnp.square(
            jax.nn.relu(jnp.dot(normed_ff, weight, preferred_element_type=jnp.float32))
        ).astype(jnp.bfloat16)
        for weight in (forward[:, :early], late_up.reshape(-1, late_width))
    ]
    lowered_part = lax.dot_general(
        jnp.concatenate(lifted, axis=1), forward[:, early:], across, preferred_element_type=jnp.float32
    )
    lowered = summed_rows(lowered_part)
    return all_rows(
        (stream.astype(jnp.float32) + root_norm(lowered, out_gain)).astype(
            jnp.bfloat16
        )
    )


def solution(mesh):
    split = Mesh(mesh.devices.reshape(4, 4, 4, 4, 2), ("zh", "zl", "y", "x", "c"))
    placed = (
        P(FS, None),
        P(),
        P(FS, TP),
        P(FS, TP),
        P(None, TP),
        P(None, TP, None, None),
        P(None, TP, None, None),
        P(None, TP),
        P(None, FS, TP),
        P(TP, FS),
        P(),
        P(),
        P(FS, TP),
        P(TP, FS),
        P(),
    )
    return jax.shard_map(
        per_device, mesh=split, in_specs=placed, out_specs=P(FS, None), check_vma=False
    )
```

```python
import jax
import jax.numpy as jnp
from jax import lax
from jax.experimental import pallas as pl
from jax.experimental.pallas import tpu as pltpu
from jax.sharding import Mesh
from jax.sharding import PartitionSpec as P

FS = ("zh", "zl", "y")
Z = ("zh", "zl")
TP = ("x", "c")


EPS = 1e-06
GATE_STEEPNESS = 8.0


def spread(array, axis):
    copies = jnp.broadcast_to(array, (lax.axis_size(axis), *array.shape))
    return lax.all_to_all(copies, axis, split_axis=0, concat_axis=0, tiled=True)


def in_order(pieces, rows):
    width = pieces.shape[-1]
    pieces = pieces.reshape(pieces.shape[0], -1, rows, width)
    return jnp.transpose(pieces, (1, 0, 2, 3)).reshape(-1, width)


def sent_round(array, axis):
    size = lax.axis_size(axis)
    pieces = [array]
    for step in range(1, size):
        ring = [(i, (i + step) % size) for i in range(size)]
        pieces.append(lax.ppermute(array, axis, ring))
    return pieces


def set_in(out, piece, place):
    deep, _, rows, width = out.shape
    nought = jnp.uint32(0)
    block = piece.reshape(deep, 1, rows, width)
    return lax.dynamic_update_slice(out, block, (nought, place, nought, nought))


def feedforward_weights(array):
    near = spread(array, "y").reshape(-1, array.shape[-1])
    return lax.all_gather(near, Z, axis=0, tiled=True)


CORES = [(0, 1), (1, 0)]


def summed_rows(rows_of, mine, others):
    sent = lax.ppermute(rows_of(others).astype(jnp.bfloat16), "c", CORES)
    kept = lax.optimization_barrier(rows_of(mine))
    half = (kept + sent.astype(jnp.float32)).astype(jnp.bfloat16)
    wide = lax.axis_size("x")
    quarters = half.reshape(wide, half.shape[0] // wide, half.shape[1])
    several = lax.all_to_all(quarters, "x", split_axis=0, concat_axis=0, tiled=True)
    return jnp.sum(several.astype(jnp.float32), axis=0)


def all_rows(part):
    half = spread(part, "x").reshape(-1, part.shape[-1])
    other = lax.ppermute(half, "c", CORES)
    mine = lax.broadcasted_iota(jnp.int32, (2, 1, 1), 0) == lax.axis_index("c")
    return jnp.where(mine, half[None], other[None]).reshape(-1, part.shape[-1])


def root_norm(values, gain):
    return (
        values
        * lax.rsqrt(jnp.mean(values * values, axis=-1, keepdims=True) + EPS)
        * gain.astype(jnp.float32)
    )


def swept(decay, drive, backward):
    length = decay.shape[0]
    place = lax.broadcasted_iota(jnp.int32, decay.shape, 0)
    step = 1
    while step < length:
        if step % 8:
            turn = length - step if backward else step
            inside = place < length - step if backward else place >= step
            far_decay = jnp.where(inside, pltpu.roll(decay, turn, 0), 1.0)
            far_drive = jnp.where(inside, pltpu.roll(drive, turn, 0), 0.0)
        else:
            one = jnp.ones((step, decay.shape[1]), jnp.float32)
            if backward:
                far_decay = jnp.concatenate((decay[step:], one), axis=0)
                far_drive = jnp.concatenate((drive[step:], 0.0 * one), axis=0)
            else:
                far_decay = jnp.concatenate((one, decay[:-step]), axis=0)
                far_drive = jnp.concatenate((0.0 * one, drive[:-step]), axis=0)
        drive = drive + decay * far_drive
        decay = decay * far_decay
        step *= 2
    return drive


def shifted(values, by):
    if by == 0:
        return values
    length = values.shape[0]
    place = lax.broadcasted_iota(jnp.int32, values.shape, 0)
    inside = place >= by if by > 0 else place < length + by
    return jnp.where(inside, pltpu.roll(values, by % length, 0), 0.0)


def one_less_exp(x):
    series = jnp.ones(x.shape, jnp.float32)
    for degree in range(8, 1, -1):
        series = 1.0 + x * series * (1.0 / degree)
    return jnp.where(jnp.abs(x) < 0.4, -x * series, 1.0 - jnp.exp(x))


def hidden_kernel(both, taps, retention, admission, rate, extra, out):
    channels = out.shape[1]
    signal = both[:, :channels].astype(jnp.float32)
    width_taps = taps.shape[0]
    total = jnp.zeros(signal.shape, jnp.float32)
    for offset in range(width_taps):
        total = total + shifted(signal, width_taps // 2 - offset) * taps[offset : offset + 1, :]
    conv_out = total.astype(jnp.bfloat16)
    wide = conv_out.astype(jnp.float32)
    state = jnp.zeros(signal.shape, jnp.float32)
    for way in range(2):
        retain = jax.nn.sigmoid(
            jnp.dot(conv_out, retention[way], preferred_element_type=jnp.float32)
        )
        admit = jax.nn.sigmoid(
            jnp.dot(conv_out, admission[way], preferred_element_type=jnp.float32)
        )
        log_decay = -GATE_STEEPNESS * retain * rate[way : way + 1, :] + extra[way]
        drive = jnp.sqrt(one_less_exp(2.0 * log_decay)) * (admit * wide)
        state = state + swept(jnp.exp(log_decay), drive, way == 1)
    out[...] = (state * jax.nn.gelu(both[:, channels:].astype(jnp.float32))).astype(out.dtype)


def per_device(
    tokens,
    recurrent_input_gain,
    recurrent_branch_weight,
    output_gate_weight,
    filter_taps,
    retention_gate_blocks,
    input_gate_blocks,
    channel_decay_rate,
    position_log_decay,
    recurrent_output_weight,
    recurrent_output_gain,
    feedforward_norm_gain,
    feedforward_up_weight,
    feedforward_down_weight,
    feedforward_output_gain,
):
    channels = recurrent_branch_weight.shape[1]
    hidden_units = feedforward_up_weight.shape[1]
    rows = recurrent_branch_weight.shape[0]
    early = hidden_units - channels
    lowest = jnp.array(-jnp.inf, jnp.bfloat16)
    down_rows = feedforward_down_weight.T
    fed = jnp.maximum(
        lax.pad(down_rows, lowest, ((0, 0, 0), (0, early, 0))),
        lax.pad(feedforward_up_weight, lowest, ((0, 0, 0), (hidden_units, early - hidden_units, 0))),
    )
    forward = feedforward_weights(fed)
    column = lax.all_gather(
        jnp.concatenate(
            (
                recurrent_branch_weight,
                output_gate_weight,
                recurrent_output_weight.T,
                feedforward_up_weight[:, early:],
            ),
            axis=1,
        ),
        Z,
        axis=0,
        tiled=True,
    )
    mixer = spread(column[:, : 3 * channels], "y")
    late, mixer = lax.optimization_barrier((column[:, 3 * channels :], mixer))
    late = sent_round(late, "y")
    mixer = in_order(mixer, rows)
    normed = lax.optimization_barrier(
        root_norm(tokens.astype(jnp.float32), recurrent_input_gain).astype(jnp.bfloat16)
    )
    both = jnp.dot(
        normed, mixer[:, : 2 * channels], preferred_element_type=jnp.float32
    ).astype(jnp.bfloat16)
    hidden = pl.pallas_call(
        hidden_kernel, out_shape=jax.ShapeDtypeStruct((both.shape[0], channels), jnp.bfloat16)
    )(
        both,
        filter_taps.astype(jnp.float32),
        retention_gate_blocks.reshape(2, channels, channels),
        input_gate_blocks.reshape(2, channels, channels),
        channel_decay_rate,
        position_log_decay,
    )
    across = (((1,), (1,)), ((), ()))

    share = tokens.shape[0] // lax.axis_size(TP)
    place = lax.axis_index("c") * lax.axis_size("x") + lax.axis_index("x")
    own = lax.dynamic_slice_in_dim(tokens, place * share, share, axis=0)
    span = lax.axis_size("y")
    turn = lax.axis_index("y").astype(jnp.uint32)
    places = [(turn + (span - step)) % span for step in range(span)]
    late_width = late[0].shape[1]
    late_up = jnp.zeros((late[0].shape[0] // rows, span, rows, late_width), jnp.bfloat16)
    late_up = set_in(late_up, late[0], places[0])
    late_up, places, own, hidden, mixer_gain, norm_gain, out_gain = lax.optimization_barrier(
        (
            late_up,
            places,
            own,
            hidden,
            recurrent_output_gain.astype(jnp.float32),
            feedforward_norm_gain.astype(jnp.float32),
            feedforward_output_gain.astype(jnp.float32),
        )
    )
    part_rows = tokens.shape[0] // 2
    core = lax.axis_index("c").astype(jnp.uint32)
    mixed = summed_rows(
        lambda these: lax.dot_general(
            these, mixer[:, 2 * channels :], across, preferred_element_type=jnp.float32
        ),
        lax.dynamic_slice_in_dim(hidden, core * part_rows, part_rows, axis=0),
        lax.dynamic_slice_in_dim(hidden, (1 - core) * part_rows, part_rows, axis=0),
    )
    stream = lax.optimization_barrier(
        (own.astype(jnp.float32) + root_norm(mixed, mixer_gain)).astype(jnp.bfloat16)
    )
    half = spread(root_norm(stream.astype(jnp.float32), norm_gain).astype(jnp.bfloat16), "x")
    half = lax.optimization_barrier(half)
    half = half.reshape(part_rows, -1)
    normed_ff = jnp.concatenate((half, lax.ppermute(half, "c", CORES)), axis=0)
    for piece, spot in zip(late[1:], places[1:]):
        late_up = set_in(late_up, piece, spot)
    lifted = [
        jnp.square(
            jax.nn.relu(jnp.dot(normed_ff, weight, preferred_element_type=jnp.float32))
        ).astype(jnp.bfloat16)
        for weight in (forward[:, hidden_units:], late_up.reshape(-1, late_width))
    ]
    lifted = jnp.concatenate(lifted, axis=1)
    lowered = summed_rows(
        lambda these: lax.dot_general(
            these, forward[:, :hidden_units], across, preferred_element_type=jnp.float32
        ),
        lifted[:part_rows],
        lifted[part_rows:],
    )
    return all_rows(
        (stream.astype(jnp.float32) + root_norm(lowered, out_gain)).astype(
            jnp.bfloat16
        )
    )


def solution(mesh):
    split = Mesh(mesh.devices.reshape(4, 4, 4, 4, 2), ("zh", "zl", "y", "x", "c"))
    placed = (
        P(FS, None),
        P(),
        P(FS, TP),
        P(FS, TP),
        P(None, TP),
        P(None, TP, None, None),
        P(None, TP, None, None),
        P(None, TP),
        P(None, FS, TP),
        P(TP, FS),
        P(),
        P(),
        P(FS, TP),
        P(TP, FS),
        P(),
    )
    return jax.shard_map(
        per_device, mesh=split, in_specs=placed, out_specs=P(FS, None), check_vma=False
    )
```

```python
import jax
import jax.numpy as jnp
from jax import lax
from jax.experimental import pallas as pl
from jax.experimental.pallas import tpu as pltpu
from jax.sharding import Mesh
from jax.sharding import PartitionSpec as P

FS = ("zh", "zl", "y")
Z = ("zh", "zl")
TP = ("x", "c")


EPS = 1e-06
GATE_STEEPNESS = 8.0


def spread(array, axis):
    copies = jnp.broadcast_to(array, (lax.axis_size(axis), *array.shape))
    return lax.all_to_all(copies, axis, split_axis=0, concat_axis=0, tiled=True)


def in_order(pieces, rows):
    width = pieces.shape[-1]
    pieces = pieces.reshape(pieces.shape[0], -1, rows, width)
    return jnp.transpose(pieces, (1, 0, 2, 3)).reshape(-1, width)


def sent_round(array, axis):
    size = lax.axis_size(axis)
    pieces = [array]
    for step in range(1, size):
        ring = [(i, (i + step) % size) for i in range(size)]
        pieces.append(lax.ppermute(array, axis, ring))
    return pieces


def set_in(out, piece, place):
    deep, _, rows, width = out.shape
    nought = jnp.uint32(0)
    block = piece.reshape(deep, 1, rows, width)
    return lax.dynamic_update_slice(out, block, (nought, place, nought, nought))


def feedforward_weights(array):
    near = spread(array, "y").reshape(-1, array.shape[-1])
    return lax.all_gather(near, Z, axis=0, tiled=True)


CORES = [(0, 1), (1, 0)]


def summed_rows(rows_of, mine, others):
    sent = lax.ppermute(rows_of(others).astype(jnp.bfloat16), "c", CORES)
    kept = lax.optimization_barrier(rows_of(mine))
    half = (kept + sent.astype(jnp.float32)).astype(jnp.bfloat16)
    wide = lax.axis_size("x")
    quarters = half.reshape(wide, half.shape[0] // wide, half.shape[1])
    several = lax.all_to_all(quarters, "x", split_axis=0, concat_axis=0, tiled=True)
    return jnp.sum(several.astype(jnp.float32), axis=0)


def all_rows(part):
    half = spread(part, "x").reshape(-1, part.shape[-1])
    other = lax.ppermute(half, "c", CORES)
    mine = lax.broadcasted_iota(jnp.int32, (2, 1, 1), 0) == lax.axis_index("c")
    return jnp.where(mine, half[None], other[None]).reshape(-1, part.shape[-1])


def root_norm(values, gain):
    return (
        values
        * lax.rsqrt(jnp.mean(values * values, axis=-1, keepdims=True) + EPS)
        * gain.astype(jnp.float32)
    )


def swept(decay, drive, backward):
    length = decay.shape[0]
    place = lax.broadcasted_iota(jnp.int32, decay.shape, 0)
    step = 1
    while step < length:
        if step % 8:
            turn = length - step if backward else step
            inside = place < length - step if backward else place >= step
            far_decay = jnp.where(inside, pltpu.roll(decay, turn, 0), 1.0)
            far_drive = jnp.where(inside, pltpu.roll(drive, turn, 0), 0.0)
        else:
            one = jnp.ones((step, decay.shape[1]), jnp.float32)
            if backward:
                far_decay = jnp.concatenate((decay[step:], one), axis=0)
                far_drive = jnp.concatenate((drive[step:], 0.0 * one), axis=0)
            else:
                far_decay = jnp.concatenate((one, decay[:-step]), axis=0)
                far_drive = jnp.concatenate((0.0 * one, drive[:-step]), axis=0)
        drive = drive + decay * far_drive
        decay = decay * far_decay
        step *= 2
    return drive


def shifted(values, by):
    if by == 0:
        return values
    length = values.shape[0]
    place = lax.broadcasted_iota(jnp.int32, values.shape, 0)
    inside = place >= by if by > 0 else place < length + by
    return jnp.where(inside, pltpu.roll(values, by % length, 0), 0.0)


def one_less_exp(x):
    series = jnp.ones(x.shape, jnp.float32)
    for degree in range(8, 1, -1):
        series = 1.0 + x * series * (1.0 / degree)
    return jnp.where(jnp.abs(x) < 0.4, -x * series, 1.0 - jnp.exp(x))


def hidden_kernel(both, taps, retention, admission, rate, extra, out):
    channels = out.shape[1]
    signal = both[:, :channels].astype(jnp.float32)
    width_taps = taps.shape[0]
    total = jnp.zeros(signal.shape, jnp.float32)
    for offset in range(width_taps):
        total = total + shifted(signal, width_taps // 2 - offset) * taps[offset : offset + 1, :]
    conv_out = total.astype(jnp.bfloat16)
    wide = conv_out.astype(jnp.float32)
    state = jnp.zeros(signal.shape, jnp.float32)
    for way in range(2):
        retain = jax.nn.sigmoid(
            jnp.dot(conv_out, retention[way], preferred_element_type=jnp.float32)
        )
        admit = jax.nn.sigmoid(
            jnp.dot(conv_out, admission[way], preferred_element_type=jnp.float32)
        )
        log_decay = -GATE_STEEPNESS * retain * rate[way : way + 1, :] + extra[way]
        drive = jnp.sqrt(one_less_exp(2.0 * log_decay)) * (admit * wide)
        state = state + swept(jnp.exp(log_decay), drive, way == 1)
    out[...] = (state * jax.nn.gelu(both[:, channels:].astype(jnp.float32))).astype(out.dtype)


def per_device(
    tokens,
    recurrent_input_gain,
    recurrent_branch_weight,
    output_gate_weight,
    filter_taps,
    retention_gate_blocks,
    input_gate_blocks,
    channel_decay_rate,
    position_log_decay,
    recurrent_output_weight,
    recurrent_output_gain,
    feedforward_norm_gain,
    feedforward_up_weight,
    feedforward_down_weight,
    feedforward_output_gain,
):
    channels = recurrent_branch_weight.shape[1]
    hidden_units = feedforward_up_weight.shape[1]
    rows = recurrent_branch_weight.shape[0]
    early = hidden_units - 2 * channels
    lowest = jnp.array(-jnp.inf, jnp.bfloat16)
    down_rows = feedforward_down_weight.T
    fed = jnp.maximum(
        lax.pad(down_rows, lowest, ((0, 0, 0), (0, early, 0))),
        lax.pad(feedforward_up_weight, lowest, ((0, 0, 0), (hidden_units, early - hidden_units, 0))),
    )
    forward = feedforward_weights(fed)
    column = lax.all_gather(
        jnp.concatenate(
            (
                recurrent_branch_weight,
                output_gate_weight,
                recurrent_output_weight.T,
                feedforward_up_weight[:, early:],
            ),
            axis=1,
        ),
        Z,
        axis=0,
        tiled=True,
    )
    mixer = spread(column[:, : 3 * channels], "y")
    late, mixer = lax.optimization_barrier((column[:, 3 * channels :], mixer))
    late = sent_round(late, "y")
    mixer = in_order(mixer, rows)
    normed = lax.optimization_barrier(
        root_norm(tokens.astype(jnp.float32), recurrent_input_gain).astype(jnp.bfloat16)
    )
    both = jnp.dot(
        normed, mixer[:, : 2 * channels], preferred_element_type=jnp.float32
    ).astype(jnp.bfloat16)
    hidden = pl.pallas_call(
        hidden_kernel, out_shape=jax.ShapeDtypeStruct((both.shape[0], channels), jnp.bfloat16)
    )(
        both,
        filter_taps.astype(jnp.float32),
        retention_gate_blocks.reshape(2, channels, channels),
        input_gate_blocks.reshape(2, channels, channels),
        channel_decay_rate,
        position_log_decay,
    )
    across = (((1,), (1,)), ((), ()))

    share = tokens.shape[0] // lax.axis_size(TP)
    place = lax.axis_index("c") * lax.axis_size("x") + lax.axis_index("x")
    own = lax.dynamic_slice_in_dim(tokens, place * share, share, axis=0)
    span = lax.axis_size("y")
    turn = lax.axis_index("y").astype(jnp.uint32)
    places = [(turn + (span - step)) % span for step in range(span)]
    late_width = late[0].shape[1]
    late_up = jnp.zeros((late[0].shape[0] // rows, span, rows, late_width), jnp.bfloat16)
    places, own, hidden, mixer_gain, norm_gain, out_gain = lax.optimization_barrier(
        (
            places,
            own,
            hidden,
            recurrent_output_gain.astype(jnp.float32),
            feedforward_norm_gain.astype(jnp.float32),
            feedforward_output_gain.astype(jnp.float32),
        )
    )
    part_rows = tokens.shape[0] // 2
    core = lax.axis_index("c").astype(jnp.uint32)
    mixed = summed_rows(
        lambda these: lax.dot_general(
            these, mixer[:, 2 * channels :], across, preferred_element_type=jnp.float32
        ),
        lax.dynamic_slice_in_dim(hidden, core * part_rows, part_rows, axis=0),
        lax.dynamic_slice_in_dim(hidden, (1 - core) * part_rows, part_rows, axis=0),
    )
    stream = lax.optimization_barrier(
        (own.astype(jnp.float32) + root_norm(mixed, mixer_gain)).astype(jnp.bfloat16)
    )
    half = spread(root_norm(stream.astype(jnp.float32), norm_gain).astype(jnp.bfloat16), "x")
    half = lax.optimization_barrier(half)
    half = half.reshape(part_rows, -1)
    normed_ff = jnp.concatenate((half, lax.ppermute(half, "c", CORES)), axis=0)
    for piece, spot in zip(late, places):
        late_up = set_in(late_up, piece, spot)
    lifted = [
        jnp.square(
            jax.nn.relu(jnp.dot(normed_ff, weight, preferred_element_type=jnp.float32))
        ).astype(jnp.bfloat16)
        for weight in (forward[:, hidden_units:], late_up.reshape(-1, late_width))
    ]
    lifted = jnp.concatenate(lifted, axis=1)
    lowered = summed_rows(
        lambda these: lax.dot_general(
            these, forward[:, :hidden_units], across, preferred_element_type=jnp.float32
        ),
        lifted[:part_rows],
        lifted[part_rows:],
    )
    return all_rows(
        (stream.astype(jnp.float32) + root_norm(lowered, out_gain)).astype(
            jnp.bfloat16
        )
    )


def solution(mesh):
    split = Mesh(mesh.devices.reshape(4, 4, 4, 4, 2), ("zh", "zl", "y", "x", "c"))
    placed = (
        P(FS, None),
        P(),
        P(FS, TP),
        P(FS, TP),
        P(None, TP),
        P(None, TP, None, None),
        P(None, TP, None, None),
        P(None, TP),
        P(None, FS, TP),
        P(TP, FS),
        P(),
        P(),
        P(FS, TP),
        P(TP, FS),
        P(),
    )
    return jax.shard_map(
        per_device, mesh=split, in_specs=placed, out_specs=P(FS, None), check_vma=False
    )
```

```python
import jax
import jax.numpy as jnp
from jax import lax
from jax.experimental import pallas as pl
from jax.experimental.pallas import tpu as pltpu
from jax.sharding import Mesh
from jax.sharding import PartitionSpec as P

FS = ("zh", "zl", "y")
Z = ("zh", "zl")
TP = ("x", "c")


EPS = 1e-06
GATE_STEEPNESS = 8.0


def spread(array, axis):
    copies = jnp.broadcast_to(array, (lax.axis_size(axis), *array.shape))
    return lax.all_to_all(copies, axis, split_axis=0, concat_axis=0, tiled=True)


def in_order(pieces, rows):
    width = pieces.shape[-1]
    pieces = pieces.reshape(pieces.shape[0], -1, rows, width)
    return jnp.transpose(pieces, (1, 0, 2, 3)).reshape(-1, width)


def sent_round(array, axis):
    size = lax.axis_size(axis)
    pieces = [array]
    for step in range(1, size):
        ring = [(i, (i + step) % size) for i in range(size)]
        pieces.append(lax.ppermute(array, axis, ring))
    return pieces


def set_in(out, piece, place):
    deep, _, rows, width = out.shape
    nought = jnp.uint32(0)
    block = piece.reshape(deep, 1, rows, width)
    return lax.dynamic_update_slice(out, block, (nought, place, nought, nought))


def feedforward_weights(array):
    near = spread(array, "y").reshape(-1, array.shape[-1])
    return lax.all_gather(near, Z, axis=0, tiled=True)


CORES = [(0, 1), (1, 0)]


def summed_rows(rows_of, mine, others):
    sent = lax.ppermute(rows_of(others).astype(jnp.bfloat16), "c", CORES)
    kept = lax.optimization_barrier(rows_of(mine))
    half = (kept + sent.astype(jnp.float32)).astype(jnp.bfloat16)
    wide = lax.axis_size("x")
    quarters = half.reshape(wide, half.shape[0] // wide, half.shape[1])
    several = lax.all_to_all(quarters, "x", split_axis=0, concat_axis=0, tiled=True)
    return jnp.sum(several.astype(jnp.float32), axis=0)


def all_rows(part):
    half = spread(part, "x").reshape(-1, part.shape[-1])
    other = lax.ppermute(half, "c", CORES)
    mine = lax.broadcasted_iota(jnp.int32, (2, 1, 1), 0) == lax.axis_index("c")
    return jnp.where(mine, half[None], other[None]).reshape(-1, part.shape[-1])


def root_norm(values, gain):
    return (
        values
        * lax.rsqrt(jnp.mean(values * values, axis=-1, keepdims=True) + EPS)
        * gain.astype(jnp.float32)
    )


def swept(decay, drive, backward):
    length = decay.shape[0]
    place = lax.broadcasted_iota(jnp.int32, decay.shape, 0)
    step = 1
    while step < length:
        if step % 8:
            turn = length - step if backward else step
            inside = place < length - step if backward else place >= step
            far_decay = jnp.where(inside, pltpu.roll(decay, turn, 0), 1.0)
            far_drive = jnp.where(inside, pltpu.roll(drive, turn, 0), 0.0)
        else:
            one = jnp.ones((step, decay.shape[1]), jnp.float32)
            if backward:
                far_decay = jnp.concatenate((decay[step:], one), axis=0)
                far_drive = jnp.concatenate((drive[step:], 0.0 * one), axis=0)
            else:
                far_decay = jnp.concatenate((one, decay[:-step]), axis=0)
                far_drive = jnp.concatenate((0.0 * one, drive[:-step]), axis=0)
        drive = drive + decay * far_drive
        decay = decay * far_decay
        step *= 2
    return drive


def shifted(values, by):
    if by == 0:
        return values
    length = values.shape[0]
    place = lax.broadcasted_iota(jnp.int32, values.shape, 0)
    inside = place >= by if by > 0 else place < length + by
    return jnp.where(inside, pltpu.roll(values, by % length, 0), 0.0)


def one_less_exp(x):
    series = jnp.ones(x.shape, jnp.float32)
    for degree in range(8, 1, -1):
        series = 1.0 + x * series * (1.0 / degree)
    return jnp.where(jnp.abs(x) < 0.4, -x * series, 1.0 - jnp.exp(x))


def hidden_kernel(both, taps, retention, admission, rate, extra, out):
    channels = out.shape[1]
    signal = both[:, :channels].astype(jnp.float32)
    width_taps = taps.shape[0]
    total = jnp.zeros(signal.shape, jnp.float32)
    for offset in range(width_taps):
        total = total + shifted(signal, width_taps // 2 - offset) * taps[offset : offset + 1, :]
    conv_out = total.astype(jnp.bfloat16)
    wide = conv_out.astype(jnp.float32)
    state = jnp.zeros(signal.shape, jnp.float32)
    for way in range(2):
        retain = jax.nn.sigmoid(
            jnp.dot(conv_out, retention[way], preferred_element_type=jnp.float32)
        )
        admit = jax.nn.sigmoid(
            jnp.dot(conv_out, admission[way], preferred_element_type=jnp.float32)
        )
        log_decay = -GATE_STEEPNESS * retain * rate[way : way + 1, :] + extra[way]
        drive = jnp.sqrt(one_less_exp(2.0 * log_decay)) * (admit * wide)
        state = state + swept(jnp.exp(log_decay), drive, way == 1)
    out[...] = (state * jax.nn.gelu(both[:, channels:].astype(jnp.float32))).astype(out.dtype)


def per_device(
    tokens,
    recurrent_input_gain,
    recurrent_branch_weight,
    output_gate_weight,
    filter_taps,
    retention_gate_blocks,
    input_gate_blocks,
    channel_decay_rate,
    position_log_decay,
    recurrent_output_weight,
    recurrent_output_gain,
    feedforward_norm_gain,
    feedforward_up_weight,
    feedforward_down_weight,
    feedforward_output_gain,
):
    channels = recurrent_branch_weight.shape[1]
    hidden_units = feedforward_up_weight.shape[1]
    rows = recurrent_branch_weight.shape[0]
    early = hidden_units - 2 * channels
    lowest = jnp.array(-jnp.inf, jnp.bfloat16)
    down_rows = feedforward_down_weight.T
    fed = jnp.maximum(
        lax.pad(down_rows, lowest, ((0, 0, 0), (0, early, 0))),
        lax.pad(feedforward_up_weight, lowest, ((0, 0, 0), (hidden_units, early - hidden_units, 0))),
    )
    forward = feedforward_weights(fed)
    column = lax.all_gather(
        jnp.concatenate(
            (
                recurrent_branch_weight,
                output_gate_weight,
                recurrent_output_weight.T,
                feedforward_up_weight[:, early:],
            ),
            axis=1,
        ),
        Z,
        axis=0,
        tiled=True,
    )
    span = lax.axis_size("y")
    turn = lax.axis_index("y").astype(jnp.uint32)
    places = [(turn + (span - step)) % span for step in range(span)]
    mixer = spread(column[:, : 2 * channels], "y")
    out_pieces = sent_round(column[:, 2 * channels : 3 * channels], "y")
    late, mixer = lax.optimization_barrier((column[:, 3 * channels :], mixer))
    late = sent_round(late, "y")
    mixer = in_order(mixer, rows)
    normed = lax.optimization_barrier(
        root_norm(tokens.astype(jnp.float32), recurrent_input_gain).astype(jnp.bfloat16)
    )
    both = jnp.dot(
        normed, mixer, preferred_element_type=jnp.float32
    ).astype(jnp.bfloat16)
    hidden = pl.pallas_call(
        hidden_kernel, out_shape=jax.ShapeDtypeStruct((both.shape[0], channels), jnp.bfloat16)
    )(
        both,
        filter_taps.astype(jnp.float32),
        retention_gate_blocks.reshape(2, channels, channels),
        input_gate_blocks.reshape(2, channels, channels),
        channel_decay_rate,
        position_log_decay,
    )
    out_rows = jnp.zeros((out_pieces[0].shape[0] // rows, span, rows, channels), jnp.bfloat16)
    for piece, spot in zip(out_pieces, places):
        out_rows = set_in(out_rows, piece, spot)
    out_rows = out_rows.reshape(-1, channels)
    across = (((1,), (1,)), ((), ()))

    share = tokens.shape[0] // lax.axis_size(TP)
    place = lax.axis_index("c") * lax.axis_size("x") + lax.axis_index("x")
    own = lax.dynamic_slice_in_dim(tokens, place * share, share, axis=0)
    late_width = late[0].shape[1]
    late_up = jnp.zeros((late[0].shape[0] // rows, span, rows, late_width), jnp.bfloat16)
    places, own, hidden, mixer_gain, norm_gain, out_gain = lax.optimization_barrier(
        (
            places,
            own,
            hidden,
            recurrent_output_gain.astype(jnp.float32),
            feedforward_norm_gain.astype(jnp.float32),
            feedforward_output_gain.astype(jnp.float32),
        )
    )
    part_rows = tokens.shape[0] // 2
    core = lax.axis_index("c").astype(jnp.uint32)
    mixed = summed_rows(
        lambda these: lax.dot_general(
            these, out_rows, across, preferred_element_type=jnp.float32
        ),
        lax.dynamic_slice_in_dim(hidden, core * part_rows, part_rows, axis=0),
        lax.dynamic_slice_in_dim(hidden, (1 - core) * part_rows, part_rows, axis=0),
    )
    stream = lax.optimization_barrier(
        (own.astype(jnp.float32) + root_norm(mixed, mixer_gain)).astype(jnp.bfloat16)
    )
    half = spread(root_norm(stream.astype(jnp.float32), norm_gain).astype(jnp.bfloat16), "x")
    half = lax.optimization_barrier(half)
    half = half.reshape(part_rows, -1)
    normed_ff = jnp.concatenate((half, lax.ppermute(half, "c", CORES)), axis=0)
    for piece, spot in zip(late, places):
        late_up = set_in(late_up, piece, spot)
    lifted = [
        jnp.square(
            jax.nn.relu(jnp.dot(normed_ff, weight, preferred_element_type=jnp.float32))
        ).astype(jnp.bfloat16)
        for weight in (forward[:, hidden_units:], late_up.reshape(-1, late_width))
    ]
    lifted = jnp.concatenate(lifted, axis=1)
    lowered = summed_rows(
        lambda these: lax.dot_general(
            these, forward[:, :hidden_units], across, preferred_element_type=jnp.float32
        ),
        lifted[:part_rows],
        lifted[part_rows:],
    )
    return all_rows(
        (stream.astype(jnp.float32) + root_norm(lowered, out_gain)).astype(
            jnp.bfloat16
        )
    )


def solution(mesh):
    split = Mesh(mesh.devices.reshape(4, 4, 4, 4, 2), ("zh", "zl", "y", "x", "c"))
    placed = (
        P(FS, None),
        P(),
        P(FS, TP),
        P(FS, TP),
        P(None, TP),
        P(None, TP, None, None),
        P(None, TP, None, None),
        P(None, TP),
        P(None, FS, TP),
        P(TP, FS),
        P(),
        P(),
        P(FS, TP),
        P(TP, FS),
        P(),
    )
    return jax.shard_map(
        per_device, mesh=split, in_specs=placed, out_specs=P(FS, None), check_vma=False
    )
```

```python
import jax
import jax.numpy as jnp
from jax import lax
from jax.experimental import pallas as pl
from jax.experimental.pallas import tpu as pltpu
from jax.sharding import Mesh
from jax.sharding import PartitionSpec as P

FS = ("zh", "zl", "y")
Z = ("zh", "zl")
TP = ("x", "c")


EPS = 1e-06
GATE_STEEPNESS = 8.0


def spread(array, axis):
    copies = jnp.broadcast_to(array, (lax.axis_size(axis), *array.shape))
    return lax.all_to_all(copies, axis, split_axis=0, concat_axis=0, tiled=True)


def in_order(pieces, rows):
    width = pieces.shape[-1]
    pieces = pieces.reshape(pieces.shape[0], -1, rows, width)
    return jnp.transpose(pieces, (1, 0, 2, 3)).reshape(-1, width)


def sent_round(array, axis):
    size = lax.axis_size(axis)
    pieces = [array]
    for step in range(1, size):
        ring = [(i, (i + step) % size) for i in range(size)]
        pieces.append(lax.ppermute(array, axis, ring))
    return pieces


def set_in(out, piece, place):
    deep, _, rows, width = out.shape
    nought = jnp.uint32(0)
    block = piece.reshape(deep, 1, rows, width)
    return lax.dynamic_update_slice(out, block, (nought, place, nought, nought))


def feedforward_weights(array):
    near = spread(array, "y").reshape(-1, array.shape[-1])
    return lax.all_gather(near, Z, axis=0, tiled=True)


CORES = [(0, 1), (1, 0)]


def summed_rows(rows_of, mine, others):
    sent = lax.ppermute(rows_of(others).astype(jnp.bfloat16), "c", CORES)
    kept = lax.optimization_barrier(rows_of(mine))
    half = (kept + sent.astype(jnp.float32)).astype(jnp.bfloat16)
    wide = lax.axis_size("x")
    quarters = half.reshape(wide, half.shape[0] // wide, half.shape[1])
    several = lax.all_to_all(quarters, "x", split_axis=0, concat_axis=0, tiled=True)
    return jnp.sum(several.astype(jnp.float32), axis=0)


def all_rows(part):
    half = spread(part, "x").reshape(-1, part.shape[-1])
    other = lax.ppermute(half, "c", CORES)
    core = lax.axis_index("c")
    mine = lax.broadcasted_iota(jnp.int32, (2, 1, 1), 0) == core
    out = jnp.where(mine, half[None], jnp.zeros_like(half)[None]).reshape(-1, part.shape[-1])
    place = (1 - core).astype(jnp.uint32) * half.shape[0]
    return lax.dynamic_update_slice_in_dim(lax.optimization_barrier(out), other, place, axis=0)


def root_norm(values, gain):
    return (
        values
        * lax.rsqrt(jnp.mean(values * values, axis=-1, keepdims=True) + EPS)
        * gain.astype(jnp.float32)
    )


def swept(decay, drive, backward):
    length = decay.shape[0]
    place = lax.broadcasted_iota(jnp.int32, decay.shape, 0)
    step = 1
    while step < length:
        if step % 8:
            turn = length - step if backward else step
            inside = place < length - step if backward else place >= step
            far_decay = jnp.where(inside, pltpu.roll(decay, turn, 0), 1.0)
            far_drive = jnp.where(inside, pltpu.roll(drive, turn, 0), 0.0)
        else:
            one = jnp.ones((step, decay.shape[1]), jnp.float32)
            if backward:
                far_decay = jnp.concatenate((decay[step:], one), axis=0)
                far_drive = jnp.concatenate((drive[step:], 0.0 * one), axis=0)
            else:
                far_decay = jnp.concatenate((one, decay[:-step]), axis=0)
                far_drive = jnp.concatenate((0.0 * one, drive[:-step]), axis=0)
        drive = drive + decay * far_drive
        decay = decay * far_decay
        step *= 2
    return drive


def shifted(values, by):
    if by == 0:
        return values
    length = values.shape[0]
    place = lax.broadcasted_iota(jnp.int32, values.shape, 0)
    inside = place >= by if by > 0 else place < length + by
    return jnp.where(inside, pltpu.roll(values, by % length, 0), 0.0)


def one_less_exp(x):
    series = jnp.ones(x.shape, jnp.float32)
    for degree in range(8, 1, -1):
        series = 1.0 + x * series * (1.0 / degree)
    return jnp.where(jnp.abs(x) < 0.4, -x * series, 1.0 - jnp.exp(x))


def hidden_kernel(both, taps, retention, admission, rate, extra, out):
    channels = out.shape[1]
    signal = both[:, :channels].astype(jnp.float32)
    width_taps = taps.shape[0]
    total = jnp.zeros(signal.shape, jnp.float32)
    for offset in range(width_taps):
        total = total + shifted(signal, width_taps // 2 - offset) * taps[offset : offset + 1, :]
    conv_out = total.astype(jnp.bfloat16)
    wide = conv_out.astype(jnp.float32)
    state = jnp.zeros(signal.shape, jnp.float32)
    for way in range(2):
        retain = jax.nn.sigmoid(
            jnp.dot(conv_out, retention[way], preferred_element_type=jnp.float32)
        )
        admit = jax.nn.sigmoid(
            jnp.dot(conv_out, admission[way], preferred_element_type=jnp.float32)
        )
        log_decay = -GATE_STEEPNESS * retain * rate[way : way + 1, :] + extra[way]
        drive = jnp.sqrt(one_less_exp(2.0 * log_decay)) * (admit * wide)
        state = state + swept(jnp.exp(log_decay), drive, way == 1)
    out[...] = (state * jax.nn.gelu(both[:, channels:].astype(jnp.float32))).astype(out.dtype)


def per_device(
    tokens,
    recurrent_input_gain,
    recurrent_branch_weight,
    output_gate_weight,
    filter_taps,
    retention_gate_blocks,
    input_gate_blocks,
    channel_decay_rate,
    position_log_decay,
    recurrent_output_weight,
    recurrent_output_gain,
    feedforward_norm_gain,
    feedforward_up_weight,
    feedforward_down_weight,
    feedforward_output_gain,
):
    channels = recurrent_branch_weight.shape[1]
    hidden_units = feedforward_up_weight.shape[1]
    rows = recurrent_branch_weight.shape[0]
    early = hidden_units - 2 * channels
    lowest = jnp.array(-jnp.inf, jnp.bfloat16)
    down_rows = feedforward_down_weight.T
    fed = jnp.maximum(
        lax.pad(down_rows, lowest, ((0, 0, 0), (0, early, 0))),
        lax.pad(feedforward_up_weight, lowest, ((0, 0, 0), (hidden_units, early - hidden_units, 0))),
    )
    forward = feedforward_weights(fed)
    column = lax.all_gather(
        jnp.concatenate(
            (
                recurrent_branch_weight,
                output_gate_weight,
                recurrent_output_weight.T,
                feedforward_up_weight[:, early:],
            ),
            axis=1,
        ),
        Z,
        axis=0,
        tiled=True,
    )
    mixer = spread(column[:, : 3 * channels], "y")
    late, mixer = lax.optimization_barrier((column[:, 3 * channels :], mixer))
    late = sent_round(late, "y")
    mixer = in_order(mixer, rows)
    normed = lax.optimization_barrier(
        root_norm(tokens.astype(jnp.float32), recurrent_input_gain).astype(jnp.bfloat16)
    )
    both = jnp.dot(
        normed, mixer[:, : 2 * channels], preferred_element_type=jnp.float32
    ).astype(jnp.bfloat16)
    hidden = pl.pallas_call(
        hidden_kernel, out_shape=jax.ShapeDtypeStruct((both.shape[0], channels), jnp.bfloat16)
    )(
        both,
        filter_taps.astype(jnp.float32),
        retention_gate_blocks.reshape(2, channels, channels),
        input_gate_blocks.reshape(2, channels, channels),
        channel_decay_rate,
        position_log_decay,
    )
    across = (((1,), (1,)), ((), ()))

    share = tokens.shape[0] // lax.axis_size(TP)
    place = lax.axis_index("c") * lax.axis_size("x") + lax.axis_index("x")
    own = lax.dynamic_slice_in_dim(tokens, place * share, share, axis=0)
    span = lax.axis_size("y")
    turn = lax.axis_index("y").astype(jnp.uint32)
    places = [(turn + (span - step)) % span for step in range(span)]
    late_width = late[0].shape[1]
    late_up = jnp.zeros((late[0].shape[0] // rows, span, rows, late_width), jnp.bfloat16)
    places, own, hidden, mixer_gain, norm_gain, out_gain = lax.optimization_barrier(
        (
            places,
            own,
            hidden,
            recurrent_output_gain.astype(jnp.float32),
            feedforward_norm_gain.astype(jnp.float32),
            feedforward_output_gain.astype(jnp.float32),
        )
    )
    part_rows = tokens.shape[0] // 2
    core = lax.axis_index("c").astype(jnp.uint32)
    mixed = summed_rows(
        lambda these: lax.dot_general(
            these, mixer[:, 2 * channels :], across, preferred_element_type=jnp.float32
        ),
        lax.dynamic_slice_in_dim(hidden, core * part_rows, part_rows, axis=0),
        lax.dynamic_slice_in_dim(hidden, (1 - core) * part_rows, part_rows, axis=0),
    )
    stream = lax.optimization_barrier(
        (own.astype(jnp.float32) + root_norm(mixed, mixer_gain)).astype(jnp.bfloat16)
    )
    half = spread(root_norm(stream.astype(jnp.float32), norm_gain).astype(jnp.bfloat16), "x")
    half = lax.optimization_barrier(half)
    half = half.reshape(part_rows, -1)
    normed_ff = jnp.concatenate((half, lax.ppermute(half, "c", CORES)), axis=0)
    for piece, spot in zip(late, places):
        late_up = set_in(late_up, piece, spot)
    lifted = [
        jnp.square(
            jax.nn.relu(jnp.dot(normed_ff, weight, preferred_element_type=jnp.float32))
        ).astype(jnp.bfloat16)
        for weight in (forward[:, hidden_units:], late_up.reshape(-1, late_width))
    ]
    lifted = jnp.concatenate(lifted, axis=1)
    lowered = summed_rows(
        lambda these: lax.dot_general(
            these, forward[:, :hidden_units], across, preferred_element_type=jnp.float32
        ),
        lifted[:part_rows],
        lifted[part_rows:],
    )
    return all_rows(
        (stream.astype(jnp.float32) + root_norm(lowered, out_gain)).astype(
            jnp.bfloat16
        )
    )


def solution(mesh):
    split = Mesh(mesh.devices.reshape(4, 4, 4, 4, 2), ("zh", "zl", "y", "x", "c"))
    placed = (
        P(FS, None),
        P(),
        P(FS, TP),
        P(FS, TP),
        P(None, TP),
        P(None, TP, None, None),
        P(None, TP, None, None),
        P(None, TP),
        P(None, FS, TP),
        P(TP, FS),
        P(),
        P(),
        P(FS, TP),
        P(TP, FS),
        P(),
    )
    return jax.shard_map(
        per_device, mesh=split, in_specs=placed, out_specs=P(FS, None), check_vma=False
    )
```

```python
import jax
import jax.numpy as jnp
from jax import lax
from jax.experimental import pallas as pl
from jax.experimental.pallas import tpu as pltpu
from jax.sharding import Mesh
from jax.sharding import PartitionSpec as P

FS = ("zh", "zl", "y")
Z = ("zh", "zl")
TP = ("x", "c")


EPS = 1e-06
GATE_STEEPNESS = 8.0


def spread(array, axis):
    copies = jnp.broadcast_to(array, (lax.axis_size(axis), *array.shape))
    return lax.all_to_all(copies, axis, split_axis=0, concat_axis=0, tiled=True)


def in_order(pieces, rows):
    width = pieces.shape[-1]
    pieces = pieces.reshape(pieces.shape[0], -1, rows, width)
    return jnp.transpose(pieces, (1, 0, 2, 3)).reshape(-1, width)


def sent_round(array, axis):
    size = lax.axis_size(axis)
    pieces = [array]
    for step in range(1, size):
        ring = [(i, (i + step) % size) for i in range(size)]
        pieces.append(lax.ppermute(array, axis, ring))
    return pieces


def set_in(out, piece, place):
    deep, _, rows, width = out.shape
    nought = jnp.uint32(0)
    block = piece.reshape(deep, 1, rows, width)
    return lax.dynamic_update_slice(out, block, (nought, place, nought, nought))


def feedforward_weights(array):
    near = spread(array, "y").reshape(-1, array.shape[-1])
    return lax.all_gather(near, Z, axis=0, tiled=True)


CORES = [(0, 1), (1, 0)]


def summed_rows(rows_of, mine, others):
    sent = lax.ppermute(rows_of(others).astype(jnp.bfloat16), "c", CORES)
    kept = lax.optimization_barrier(rows_of(mine))
    half = (kept + sent.astype(jnp.float32)).astype(jnp.bfloat16)
    wide = lax.axis_size("x")
    quarters = half.reshape(wide, half.shape[0] // wide, half.shape[1])
    several = lax.all_to_all(quarters, "x", split_axis=0, concat_axis=0, tiled=True)
    return jnp.sum(several.astype(jnp.float32), axis=0)


def all_rows(part):
    half = spread(part, "x").reshape(-1, part.shape[-1])
    other = lax.ppermute(half, "c", CORES)
    core = lax.axis_index("c")
    mine = lax.broadcasted_iota(jnp.int32, (2, 1, 1), 0) == core
    out = jnp.where(mine, half[None], jnp.zeros_like(half)[None]).reshape(-1, part.shape[-1])
    place = (1 - core).astype(jnp.uint32) * half.shape[0]
    return lax.dynamic_update_slice_in_dim(lax.optimization_barrier(out), other, place, axis=0)


def root_norm(values, gain):
    return (
        values
        * lax.rsqrt(jnp.mean(values * values, axis=-1, keepdims=True) + EPS)
        * gain.astype(jnp.float32)
    )


def swept(decay, drive, backward):
    length = decay.shape[0]
    place = lax.broadcasted_iota(jnp.int32, decay.shape, 0)
    step = 1
    while step < length:
        if step % 8:
            turn = length - step if backward else step
            inside = place < length - step if backward else place >= step
            far_decay = jnp.where(inside, pltpu.roll(decay, turn, 0), 1.0)
            far_drive = jnp.where(inside, pltpu.roll(drive, turn, 0), 0.0)
        else:
            one = jnp.ones((step, decay.shape[1]), jnp.float32)
            if backward:
                far_decay = jnp.concatenate((decay[step:], one), axis=0)
                far_drive = jnp.concatenate((drive[step:], 0.0 * one), axis=0)
            else:
                far_decay = jnp.concatenate((one, decay[:-step]), axis=0)
                far_drive = jnp.concatenate((0.0 * one, drive[:-step]), axis=0)
        drive = drive + decay * far_drive
        decay = decay * far_decay
        step *= 2
    return drive


def shifted(values, by):
    if by == 0:
        return values
    length = values.shape[0]
    place = lax.broadcasted_iota(jnp.int32, values.shape, 0)
    inside = place >= by if by > 0 else place < length + by
    return jnp.where(inside, pltpu.roll(values, by % length, 0), 0.0)


def one_less_exp(x):
    series = jnp.ones(x.shape, jnp.float32)
    for degree in range(8, 1, -1):
        series = 1.0 + x * series * (1.0 / degree)
    return jnp.where(jnp.abs(x) < 0.4, -x * series, 1.0 - jnp.exp(x))


def hidden_kernel(normed, weights, taps, retention, admission, rate, extra, out):
    channels = out.shape[1]
    both = jnp.dot(
        normed[...], weights[:, : 2 * channels], preferred_element_type=jnp.float32
    ).astype(jnp.bfloat16)
    signal = both[:, :channels].astype(jnp.float32)
    width_taps = taps.shape[0]
    total = jnp.zeros(signal.shape, jnp.float32)
    for offset in range(width_taps):
        total = total + shifted(signal, width_taps // 2 - offset) * taps[offset : offset + 1, :]
    conv_out = total.astype(jnp.bfloat16)
    wide = conv_out.astype(jnp.float32)
    state = jnp.zeros(signal.shape, jnp.float32)
    for way in range(2):
        retain = jax.nn.sigmoid(
            jnp.dot(conv_out, retention[way], preferred_element_type=jnp.float32)
        )
        admit = jax.nn.sigmoid(
            jnp.dot(conv_out, admission[way], preferred_element_type=jnp.float32)
        )
        log_decay = -GATE_STEEPNESS * retain * rate[way : way + 1, :] + extra[way]
        drive = jnp.sqrt(one_less_exp(2.0 * log_decay)) * (admit * wide)
        state = state + swept(jnp.exp(log_decay), drive, way == 1)
    out[...] = (state * jax.nn.gelu(both[:, channels:].astype(jnp.float32))).astype(out.dtype)


def per_device(
    tokens,
    recurrent_input_gain,
    recurrent_branch_weight,
    output_gate_weight,
    filter_taps,
    retention_gate_blocks,
    input_gate_blocks,
    channel_decay_rate,
    position_log_decay,
    recurrent_output_weight,
    recurrent_output_gain,
    feedforward_norm_gain,
    feedforward_up_weight,
    feedforward_down_weight,
    feedforward_output_gain,
):
    channels = recurrent_branch_weight.shape[1]
    hidden_units = feedforward_up_weight.shape[1]
    rows = recurrent_branch_weight.shape[0]
    early = hidden_units - 2 * channels
    lowest = jnp.array(-jnp.inf, jnp.bfloat16)
    down_rows = feedforward_down_weight.T
    fed = jnp.maximum(
        lax.pad(down_rows, lowest, ((0, 0, 0), (0, early, 0))),
        lax.pad(feedforward_up_weight, lowest, ((0, 0, 0), (hidden_units, early - hidden_units, 0))),
    )
    forward = feedforward_weights(fed)
    column = lax.all_gather(
        jnp.concatenate(
            (
                recurrent_branch_weight,
                output_gate_weight,
                recurrent_output_weight.T,
                feedforward_up_weight[:, early:],
            ),
            axis=1,
        ),
        Z,
        axis=0,
        tiled=True,
    )
    mixer = spread(column[:, : 3 * channels], "y")
    late, mixer = lax.optimization_barrier((column[:, 3 * channels :], mixer))
    late = sent_round(late, "y")
    mixer = in_order(mixer, rows)
    normed = lax.optimization_barrier(
        root_norm(tokens.astype(jnp.float32), recurrent_input_gain).astype(jnp.bfloat16)
    )
    hidden = pl.pallas_call(
        hidden_kernel, out_shape=jax.ShapeDtypeStruct((tokens.shape[0], channels), jnp.bfloat16)
    )(
        normed,
        mixer,
        filter_taps.astype(jnp.float32),
        retention_gate_blocks.reshape(2, channels, channels),
        input_gate_blocks.reshape(2, channels, channels),
        channel_decay_rate,
        position_log_decay,
    )
    across = (((1,), (1,)), ((), ()))

    share = tokens.shape[0] // lax.axis_size(TP)
    place = lax.axis_index("c") * lax.axis_size("x") + lax.axis_index("x")
    own = lax.dynamic_slice_in_dim(tokens, place * share, share, axis=0)
    span = lax.axis_size("y")
    turn = lax.axis_index("y").astype(jnp.uint32)
    places = [(turn + (span - step)) % span for step in range(span)]
    late_width = late[0].shape[1]
    late_up = jnp.zeros((late[0].shape[0] // rows, span, rows, late_width), jnp.bfloat16)
    places, own, hidden, mixer_gain, norm_gain, out_gain = lax.optimization_barrier(
        (
            places,
            own,
            hidden,
            recurrent_output_gain.astype(jnp.float32),
            feedforward_norm_gain.astype(jnp.float32),
            feedforward_output_gain.astype(jnp.float32),
        )
    )
    part_rows = tokens.shape[0] // 2
    core = lax.axis_index("c").astype(jnp.uint32)
    mixed = summed_rows(
        lambda these: lax.dot_general(
            these, mixer[:, 2 * channels :], across, preferred_element_type=jnp.float32
        ),
        lax.dynamic_slice_in_dim(hidden, core * part_rows, part_rows, axis=0),
        lax.dynamic_slice_in_dim(hidden, (1 - core) * part_rows, part_rows, axis=0),
    )
    stream = lax.optimization_barrier(
        (own.astype(jnp.float32) + root_norm(mixed, mixer_gain)).astype(jnp.bfloat16)
    )
    half = spread(root_norm(stream.astype(jnp.float32), norm_gain).astype(jnp.bfloat16), "x")
    half = lax.optimization_barrier(half)
    half = half.reshape(part_rows, -1)
    normed_ff = jnp.concatenate((half, lax.ppermute(half, "c", CORES)), axis=0)
    for piece, spot in zip(late, places):
        late_up = set_in(late_up, piece, spot)
    lifted = [
        jnp.square(
            jax.nn.relu(jnp.dot(normed_ff, weight, preferred_element_type=jnp.float32))
        ).astype(jnp.bfloat16)
        for weight in (forward[:, hidden_units:], late_up.reshape(-1, late_width))
    ]
    lifted = jnp.concatenate(lifted, axis=1)
    lowered = summed_rows(
        lambda these: lax.dot_general(
            these, forward[:, :hidden_units], across, preferred_element_type=jnp.float32
        ),
        lifted[:part_rows],
        lifted[part_rows:],
    )
    return all_rows(
        (stream.astype(jnp.float32) + root_norm(lowered, out_gain)).astype(
            jnp.bfloat16
        )
    )


def solution(mesh):
    split = Mesh(mesh.devices.reshape(4, 4, 4, 4, 2), ("zh", "zl", "y", "x", "c"))
    placed = (
        P(FS, None),
        P(),
        P(FS, TP),
        P(FS, TP),
        P(None, TP),
        P(None, TP, None, None),
        P(None, TP, None, None),
        P(None, TP),
        P(None, FS, TP),
        P(TP, FS),
        P(),
        P(),
        P(FS, TP),
        P(TP, FS),
        P(),
    )
    return jax.shard_map(
        per_device, mesh=split, in_specs=placed, out_specs=P(FS, None), check_vma=False
    )
```
